256 devices in a mesh: ep: 64 (over z, y, core), tp: 4 (over x).
Axes of the slice: x: 4, y: 4, z: 8, core: 2. Of those that a mesh axis runs over, the one named last changes fastest.
Arguments:
- tokens: bfloat16 [49152, 2048], P('ep', 'tp')
- norm_gain: float32 [2048], P('tp'), may hold values from 0.1 to 1.9
- routing: int32 [49152, 2], P('ep'), may hold values from 0 to 63, as said below
- route_weight: float32 [49152, 2], P('ep'), may hold values from 0.2 to 1
- w_gate: bfloat16 [64, 2048, 512], P('ep', 'tp'), may hold values from -0.125 to 0.125
- w_up: bfloat16 [64, 2048, 512], P('ep', 'tp'), may hold values from -0.125 to 0.125
- w_down: bfloat16 [64, 512, 2048], P('ep', None, 'tp'), may hold values from -0.25 to 0.25
- w_branch_in: bfloat16 [2048, 1024], P('ep', 'tp'), may hold values from -0.125 to 0.125
- w_branch_out: bfloat16 [1024, 2048], P('tp', 'ep'), may hold values from -0.1875 to 0.1875
- branch_gate: float32 [2048], P('tp'), may hold values from -3 to 3
Outputs:
- mixed: bfloat16 [49152, 2048], P('ep', 'tp')
The draws below stay inside these ranges and needn't reach their ends.
Inputs may be any that keep to these rules, and one draw needn't show every extreme that they name: `routing`: each row names two different experts of the same group; expert e belongs to group e // 16. Among the rows of one device (aligned blocks of 768 rows) no expert is named more than 48 times, and in every block all experts of one group are named exactly 48 times.
All inputs are finite; a program needn't handle non-finite values.
Results may differ from the reference program's by a relative error of at most 0.0069.
Values may be sent and summed in bfloat16 or wider, within the bound.
A program may use at most 128 MiB of HBM per device.

```python
import math
import jax
import jax.numpy as jnp
from jax import lax

D = 2048
FF = 512
BR = 1024
GROUPS = 4
TOK_DEV = 768
EXPERTS = 64
CAP = 48
TOKENS = 49152
N_EP = 64
N_TP = 4


def draw_tokens(key, part):
    first, second = jax.random.split(key, 2)
    base = jax.random.normal(first, (TOKENS, D), jnp.float32)
    scales = jnp.exp(jax.random.uniform(second, (N_TP,), jnp.float32, math.log(0.3), math.log(3.0)))
    values = base.reshape(TOKENS, N_TP, D // N_TP) * scales[None, :, None]
    return values.reshape(TOKENS, D).astype(jnp.bfloat16)


def draw_routing(key, part):
    per_group = EXPERTS // GROUPS
    half = TOK_DEV // 2

    def one_block(block):
        block_key = jax.random.fold_in(key, block)
        keys = jax.random.split(block_key, 3 + GROUPS)
        busiest = jax.random.randint(keys[0], (), 0, GROUPS)
        cuts = jax.random.randint(keys[1], (2,), 0, half + 1)
        lower = jnp.min(cuts)
        upper = jnp.max(cuts)
        others = jnp.stack([lower, upper - lower, half - upper])
        group_ids = jnp.arange(GROUPS, dtype=jnp.int32)
        other_place = jnp.clip(group_ids - (group_ids > busiest).astype(jnp.int32), 0, 2)
        counts = jnp.where(group_ids == busiest, half, others[other_place])
        ends = jnp.cumsum(counts)
        starts = ends - counts
        position = jnp.arange(TOK_DEV, dtype=jnp.int32)
        group = jnp.sum((position[:, None] >= ends[None, :]).astype(jnp.int32), axis=1)
        local = position - starts[group]
        orders = jnp.stack([jax.random.permutation(keys[3 + g], per_group) for g in range(GROUPS)]).astype(jnp.int32)
        offset = 1 + local // per_group % (per_group - 1)
        first = orders[group, local % per_group]
        second = orders[group, (local + offset) % per_group]
        paired = jnp.stack([group * per_group + first, group * per_group + second], axis=1)
        shuffle = jax.random.permutation(keys[2], TOK_DEV)
        return paired[shuffle]
    blocks = jax.vmap(one_block)(jnp.arange(N_EP, dtype=jnp.int32))
    return blocks.reshape(TOKENS, 2).astype(jnp.int32)


def levels(rng, shape, cuts, low, high):
    def one(dim, shards_of):
        heights = jax.random.uniform(jax.random.fold_in(jax.random.fold_in(rng, 6), dim), (shards_of,), jnp.float32, low / len(cuts), high / len(cuts))
        return jnp.repeat(jnp.exp(heights), shape[dim] // shards_of).reshape((-1,) + (1,) * (len(shape) - dim - 1))

    gain = one(*cuts[0])
    for cut in cuts[1:]:
        gain = gain * one(*cut)
    return gain


def normal_values(own_key, extent, spread, most, cuts=(), held_as=jnp.bfloat16):
    level = levels(own_key, extent, cuts, -0.22, 0.18) if cuts else 1.0
    array = jax.random.normal(own_key, extent, jnp.float32) * spread * level
    return jnp.minimum(jnp.maximum(array, -most), most).astype(held_as)


def setup_inputs(seed: int = 0) -> dict:
    splits = jax.random.split(jax.random.key(seed), 11)
    return {
        "tokens": draw_tokens(jax.random.fold_in(splits[10], 71), 0),
        "norm_gain": jnp.clip(1.0 + 0.18 * jax.random.normal(splits[1], (D,), jnp.float32), 0.1, 1.9),
        "routing": draw_routing(jax.random.fold_in(splits[10], 71), 0),
        "route_weight": jnp.clip(0.2 + 0.8 * jax.random.uniform(splits[3], (TOKENS, 2), jnp.float32) ** levels(splits[3], (TOKENS, 2), ((0, 64),), -0.2, 0.2), 0.2, 1.0),
        "w_gate": normal_values(splits[4], (EXPERTS, D, FF), D ** -0.5, 0.125, ((0, 64), (1, 4))),
        "w_up": normal_values(splits[5], (EXPERTS, D, FF), D ** -0.5, 0.125, ((0, 64), (1, 4))),
        "w_down": normal_values(splits[6], (EXPERTS, FF, D), FF ** -0.5, 0.25, ((0, 64), (2, 4))),
        "w_branch_in": normal_values(splits[7], (D, BR), D ** -0.5, 0.125, ((0, 64), (1, 4))),
        "w_branch_out": normal_values(splits[8], (BR, D), BR ** -0.5, 0.1875, ((0, 4), (1, 64))),
        "branch_gate": jnp.clip(jax.random.uniform(splits[9], (D,), jnp.float32, -3.0, 3.0) * levels(splits[9], (D,), ((0, 4),), -0.4, 0.0), -3.0, 3.0),
    }


epsilon = 1e-06

def slot_numbers(routing):
    flat_ids = routing.reshape(N_EP, TOK_DEV * 2)
    one_hot = (flat_ids[:, :, None] == jnp.arange(EXPERTS, dtype=jnp.int32)[None, None, :]).astype(jnp.int32)
    before = jnp.cumsum(one_hot, axis=1) - one_hot
    return lax.optimization_barrier(jnp.sum(before * one_hot, axis=2)).reshape(TOKENS, 2).astype(jnp.int32)

def expert(operands):
    inputs, gate_weight, up_weight, down_weight = operands
    gate_sum = jnp.dot(inputs, gate_weight, preferred_element_type=jnp.float32)
    up_sum = jnp.dot(inputs, up_weight, preferred_element_type=jnp.float32)
    hidden = (jax.nn.silu(gate_sum) * up_sum).astype(jnp.bfloat16)
    return jnp.dot(hidden, down_weight, preferred_element_type=jnp.float32).astype(jnp.bfloat16)

def reference(tokens, norm_gain, routing, route_weight, w_gate, w_up, w_down, w_branch_in, w_branch_out, branch_gate):
    floats = tokens.astype(jnp.float32)
    squares = lax.optimization_barrier(jnp.mean(floats * floats, axis=1, keepdims=True))
    normed = (floats * lax.rsqrt(squares + epsilon) * norm_gain).astype(jnp.bfloat16)
    source = (jnp.arange(TOKENS, dtype=jnp.int32) // TOK_DEV)[:, None]
    place = (source * CAP + slot_numbers(routing)).astype(jnp.int32)
    copies = jnp.broadcast_to(normed[:, None, :], (TOKENS, 2, D))
    buffer = jnp.zeros((EXPERTS, N_EP * CAP, D), jnp.bfloat16).at[routing, place].set(copies)
    outputs = lax.map(expert, (buffer, w_gate, w_up, w_down))
    picked = outputs[routing, place].astype(jnp.float32)
    routed = lax.optimization_barrier(jnp.sum(picked * route_weight[:, :, None], axis=1))
    branch_hidden = jax.nn.silu(jnp.dot(normed, w_branch_in, preferred_element_type=jnp.float32)).astype(jnp.bfloat16)
    branch = jnp.dot(branch_hidden, w_branch_out, preferred_element_type=jnp.float32).astype(jnp.bfloat16)
    return (routed + jax.nn.sigmoid(branch_gate) * branch.astype(jnp.float32)).astype(jnp.bfloat16)
```

```python
import functools

import jax
import jax.numpy as jnp
from jax import lax
from jax.experimental import pallas as pl
from jax.experimental.pallas import tpu as pltpu
from jax.sharding import PartitionSpec as P

EPSILON = 1e-06
MESH = pl.DeviceIdType.MESH
CAP = 48
F = 512
T = 768
NQ = 16
BLK = 4 * CAP


def kernel(
    tok_hbm, gain_hbm, rout_t, rout, rw, wg_hbm, wu_hbm, wd_hbm, bw_hbm, gate_ref,
    out_ref,
    tok, gains, send, land, weights, bw, normed, hidden, result, ret, btok, bnorm, bhid, bres, bret, acc,
    lsem, gsend, grecv, btsend, btrecv, brsend, brrecv, zsend, zrecv, xsend, xrecv, ysend, yrecv, dsend, drecv,
    wsend, wrecv, fsend, frecv, esend, erecv, rsend, rrecv,
):
    ep = lax.axis_index("ep")
    x = lax.axis_index("tp")
    z, y, c = ep // 8, (ep // 2) % 4, ep % 2
    m_own, s4 = ep // 4, ep % 4
    is_self = x == (2 * ep) % 4
    sigma = (x - s4 + 4) % 4

    def remote(src, dst, ssem, rsem, e, xx):
        return pltpu.make_async_remote_copy(
            src_ref=src, dst_ref=dst, send_sem=ssem, recv_sem=rsem,
            device_id={"ep": e, "tp": xx}, device_id_type=MESH,
        )

    def lanes(index, width):
        return pl.ds(pl.multiple_of(index * width, width), width)

    def ep_of(zz, yy, cc):
        return (zz * 4 + yy) * 2 + cc

    loads = [
        pltpu.make_async_copy(tok_hbm, tok, lsem.at[0]),
        pltpu.make_async_copy(bw_hbm, bw.at[:, z, y, c, :, lanes(x, 256)], lsem.at[1]),
        pltpu.make_async_copy(gain_hbm, gains.at[x], lsem.at[2]),
        pltpu.make_async_copy(tok_hbm.at[pl.ds(x * 192, 192), :], btok.at[:, lanes(x, F)], lsem.at[3]),
        pltpu.make_async_copy(wg_hbm, weights.at[0, x], lsem.at[4]),
        pltpu.make_async_copy(wu_hbm, weights.at[1, x], lsem.at[5]),
        pltpu.make_async_copy(wd_hbm, weights.at[2, x], lsem.at[6]),
    ]
    for load in loads:
        load.start()
    for load in loads:
        load.wait()

    def z_copy(d):
        zz = (z + d) % 8
        mine = bw.at[:, z, y, c, :, lanes(x, 256)]
        return remote(mine, mine, zsend.at[d], zrecv.at[d], ep_of(zz, y, c), x)

    for d in range(1, 8):
        z_copy(d).start()

    def gain_copy(d):
        return remote(gains.at[x], gains.at[x], gsend.at[d], grecv.at[d], ep, (x + d) % 4)

    def btok_copy(d):
        xx = (x + d) % 4
        return remote(
            tok.at[pl.ds(xx * 192, 192), :], btok.at[:, lanes(x, F)], btsend.at[d], btrecv.at[d], ep, xx
        )

    for d in range(1, 4):
        gain_copy(d).start()

    experts = lax.broadcasted_iota(jnp.int32, (64, T), 0)
    r0, r1 = rout_t[0:1, :], rout_t[1:2, :]
    named0, named1 = experts == r0, experts == r1
    one_hot = jnp.where(named0 | named1, 1.0, 0.0).astype(jnp.bfloat16)
    earlier = jnp.where(
        lax.broadcasted_iota(jnp.int32, (T, T), 0) < lax.broadcasted_iota(jnp.int32, (T, T), 1), 1.0, 0.0
    ).astype(jnp.bfloat16)
    before = jnp.dot(one_hot, earlier, preferred_element_type=jnp.float32)
    slot0 = r0 * CAP + jnp.sum(jnp.where(named0, before, 0.0), axis=0, keepdims=True).astype(jnp.int32)
    slot1 = r1 * CAP + jnp.sum(jnp.where(named1, before, 0.0), axis=0, keepdims=True).astype(jnp.int32)

    def block_at(q):
        half = (q + 1) // 2
        return (m_own + 16 + half * (2 * (q % 2) - 1)) % 16

    def dispatch_copy(q, j):
        m, xx = block_at(q), (x + j) % 4
        r = (xx - s4 + 4) % 4
        return remote(
            send.at[m, pl.ds(pl.multiple_of(r * CAP, 16), CAP), :],
            land.at[m_own, :, lanes(x, F)],
            esend.at[q * 4 + j],
            erecv.at[m_own * 4 + x],
            m * 4 + r,
            xx,
        )

    def pack(q, carry):
        m = block_at(q)
        slots = lax.broadcasted_iota(jnp.int32, (BLK, T), 0) + m * BLK
        pick = jnp.where((slots == slot0) | (slots == slot1), 1.0, 0.0).astype(jnp.bfloat16)
        send[m] = jnp.dot(pick, tok[...], preferred_element_type=jnp.float32).astype(jnp.bfloat16)
        for j in range(4):
            if j == 0:
                own = (q == 0) & is_self

                @pl.when(jnp.logical_not(own))
                def _():
                    dispatch_copy(q, j).start()

                @pl.when(own)
                def _():
                    land[m_own, :, lanes(x, F)] = send[m_own, pl.ds(pl.multiple_of(s4 * CAP, 16), CAP), :]
            else:
                dispatch_copy(q, j).start()
        return carry

    lax.fori_loop(0, NQ, pack, 0)

    def w_copy(k, way):
        return remote(
            weights.at[k, x], weights.at[k, x], wsend.at[k, way], wrecv.at[k, way], ep, (x + (1, 3)[way]) % 4
        )

    def f_copy(k, way):
        slot = (x + (3, 1)[way]) % 4
        if k == 2:
            piece = weights.at[2, slot, pl.ds(256 * way, 256), :]
        else:
            piece = weights.at[way, slot]
        return remote(piece, piece, fsend.at[k // 2, way], frecv.at[k // 2, way], ep, (x + (1, 3)[way]) % 4)

    for k in range(3):
        for way in range(2):
            w_copy(k, way).start()
    for d in range(1, 4):
        btok_copy(d).start()

    for d in range(1, 8):
        z_copy(d).wait_recv()

    def x_copy(k, d):
        mine = bw.at[k, :, y, c, :, lanes(x, 256)]
        return remote(mine, mine, xsend.at[k, d], xrecv.at[k, d], ep, (x + d) % 4)

    for d in range(1, 4):
        for k in range(2):
            x_copy(k, d).start()
    for way in range(2):
        for k in range(2):
            w_copy(k, way).wait_recv()
    for way in range(2):
        f_copy(0, way).start()
    for way in range(2):
        w_copy(2, way).wait_recv()
    for way in range(2):
        f_copy(2, way).start()
    for d in range(1, 4):
        for k in range(2):
            x_copy(k, d).wait_recv()

    def y_copy(k, way):
        mine = bw.at[k, :, y, c]
        return remote(mine, mine, ysend.at[k, way], yrecv.at[k, way], ep_of(z, (y + (1, 3)[way]) % 4, c), x)

    def y_forward(way):
        slot = (y + (3, 1)[way]) % 4
        piece = bw.at[way, :, slot, c]
        return remote(piece, piece, ysend.at[2, way], yrecv.at[2, way], ep_of(z, (y + (1, 3)[way]) % 4, c), x)

    for way in range(2):
        for k in range(2):
            y_copy(k, way).start()

    for d in range(1, 4):
        gain_copy(d).wait_recv()
    for way in range(2):
        f_copy(0, way).wait_recv()
    for way in range(2):
        f_copy(2, way).wait_recv()

    def norm_rows(source, target):
        floats = source.astype(jnp.float32)
        squares = jnp.sum(floats * floats, axis=1, keepdims=True)
        scaled = floats * lax.rsqrt(squares * (1.0 / (4 * F)) + EPSILON)
        for k in range(4):
            target[:, k * F : (k + 1) * F] = (scaled[:, k * F : (k + 1) * F] * gains[k, 0:1, :]).astype(jnp.bfloat16)

    def arrival(m, xx):
        there = land.at[m, :, lanes(xx, F)]
        return remote(there, there, esend.at[0], erecv.at[m * 4 + xx], ep, xx)

    def return_copy(jj, m):
        quarter = (x + (0, 1, 3, 2)[jj]) % 4
        return remote(
            result.at[quarter, m], ret.at[ep], rsend.at[jj * 16 + m], rrecv.at[ep], m * 4 + sigma, quarter
        )

    def expert(i, carry):
        part = (z // 2 + i) % 4
        for mm in range(4):
            m = part * 4 + mm
            for xx in range(4):

                @pl.when(jnp.logical_not(is_self & (m == m_own) & (x == xx)))
                def _():
                    arrival(m, xx).wait_recv()

        def one(r, inner):
            m, row = part * 4 + r // 3, pl.multiple_of((r % 3) * 16, 16)
            norm_rows(land[m, pl.ds(row, 16), :], normed.at[pl.ds(pl.multiple_of(r * 16, 16), 16), :])
            return inner

        lax.fori_loop(0, 12, one, 0)
        for n in range(2):
            cols = slice(n * 256, n * 256 + 256)
            sums = []
            for k in range(2):
                total = jnp.dot(normed[:, 0:F], weights[k, 0, :, cols], preferred_element_type=jnp.float32)
                for h in range(1, 4):
                    total += jnp.dot(
                        normed[:, h * F : (h + 1) * F], weights[k, h, :, cols], preferred_element_type=jnp.float32
                    )
                sums.append(total)
            gate_sum, up_sum = sums
            hidden[:, cols] = (gate_sum / (1.0 + jnp.exp(-gate_sum)) * up_sum).astype(jnp.bfloat16)
        for jj in range(4):
            quarter = (x + (0, 1, 3, 2)[jj]) % 4
            rows = jnp.dot(hidden[...], weights[2, quarter], preferred_element_type=jnp.float32)
            result[quarter, pl.ds(part * 4, 4)] = rows.astype(jnp.bfloat16).reshape(4, CAP, F)
            for mm in range(4):
                m = part * 4 + mm
                if jj == 0:
                    own = is_self & (m == m_own)

                    @pl.when(jnp.logical_not(own))
                    def _():
                        return_copy(jj, m).start()

                    @pl.when(own)
                    def _():
                        ret[ep] = result[x, m_own]
                else:
                    return_copy(jj, m).start()
        return carry

    lax.fori_loop(0, 4, expert, 0)

    for way in range(2):
        for k in range(2):
            y_copy(k, way).wait_recv()
    for way in range(2):
        y_forward(way).start()
    for way in range(2):
        y_forward(way).wait_recv()

    def d_copy(k):
        mine = bw.at[k, :, :, c]
        return remote(mine, mine, dsend.at[k], drecv.at[k], ep_of(z, y, 1 - c), x)

    for k in range(2):
        d_copy(k).start()

    for d in range(1, 4):
        btok_copy(d).wait_recv()

    def branch_norm(r, carry):
        rows = pl.ds(pl.multiple_of(r * 16, 16), 16)
        norm_rows(btok[rows, :], bnorm.at[rows, :])
        return carry

    lax.fori_loop(0, 12, branch_norm, 0)

    lane_experts = lax.broadcasted_iota(jnp.int32, (T, 128), 1)
    c0, c1 = rout[:, 0:1], rout[:, 1:2]
    named0, named1 = lane_experts == c0, lane_experts == c1
    one_hot = jnp.where(named0 | named1, 1.0, 0.0).astype(jnp.bfloat16)
    earlier = jnp.where(
        lax.broadcasted_iota(jnp.int32, (T, T), 1) < lax.broadcasted_iota(jnp.int32, (T, T), 0), 1.0, 0.0
    ).astype(jnp.bfloat16)
    before = jnp.dot(earlier, one_hot, preferred_element_type=jnp.float32)
    place0 = c0 * CAP + jnp.sum(jnp.where(named0, before, 0.0), axis=1, keepdims=True).astype(jnp.int32)
    place1 = c1 * CAP + jnp.sum(jnp.where(named1, before, 0.0), axis=1, keepdims=True).astype(jnp.int32)

    for k in range(2):
        d_copy(k).wait_recv()

    w_in = bw.at[0].reshape(2048, 1024)
    w_out = bw.at[1].reshape(2048, 1024)
    for n in range(4):
        cols = slice(n * 256, n * 256 + 256)
        total = jnp.dot(bnorm[...], w_in[:, cols], preferred_element_type=jnp.float32)
        bhid[:, cols] = (total / (1.0 + jnp.exp(-total))).astype(jnp.bfloat16)

    def bret_copy(d):
        xx = (x + d) % 4
        return remote(
            bres.at[xx], bret.at[pl.ds(x * 192, 192), :], brsend.at[d], brrecv.at[d], ep, xx
        )

    for d in (1, 3, 2, 0):
        quarter = (x + d) % 4
        rows = lax.dot_general(
            bhid[...],
            w_out[pl.ds(pl.multiple_of(quarter * F, F), F), :],
            (((1,), (1,)), ((), ())),
            preferred_element_type=jnp.float32,
        )
        if d == 0:
            bret[pl.ds(pl.multiple_of(x * 192, 192), 192), :] = rows.astype(jnp.bfloat16)
        else:
            bres[quarter] = rows.astype(jnp.bfloat16)
            bret_copy(d).start()

    acc[...] = jnp.zeros_like(acc)

    def returned(e):
        return remote(ret.at[e], ret.at[e], rsend.at[0], rrecv.at[e], ep, x)

    def combine(i, carry):
        part = (z // 2 + i) % 4

        def wait(k, inner):
            e = part * 16 + k

            @pl.when(jnp.logical_not(is_self & (e == ep)))
            def _():
                returned(e).wait_recv()

            return inner

        lax.fori_loop(0, 16, wait, 0)
        rows = ret[pl.ds(part * 16, 16)].reshape(16 * CAP, F)
        for h in range(3):
            sl = slice(h * 256, h * 256 + 256)
            slots = lax.broadcasted_iota(jnp.int32, (256, 16 * CAP), 1) + part * (16 * CAP)
            mix = jnp.where(slots == place0[sl], rw[sl, 0:1], 0.0) + jnp.where(slots == place1[sl], rw[sl, 1:2], 0.0)
            acc[sl, :] += jnp.dot(mix.astype(jnp.bfloat16), rows, preferred_element_type=jnp.float32)
        return carry

    lax.fori_loop(0, 4, combine, 0)
    for d in range(1, 4):
        bret_copy(d).wait_recv()
    share = 1.0 / (1.0 + jnp.exp(-gate_ref[0:1, :]))
    for h in range(3):
        sl = slice(h * 256, h * 256 + 256)
        out_ref[sl, :] = (acc[sl, :] + share * bret[sl, :].astype(jnp.float32)).astype(jnp.bfloat16)

    for d in range(1, 8):
        z_copy(d).wait_send()
    for d in range(1, 4):
        gain_copy(d).wait_send()
        btok_copy(d).wait_send()
        bret_copy(d).wait_send()
        for k in range(2):
            x_copy(k, d).wait_send()
    for way in range(2):
        for k in range(3):
            w_copy(k, way).wait_send()
        for k in (0, 2):
            f_copy(k, way).wait_send()
        for k in range(2):
            y_copy(k, way).wait_send()
        y_forward(way).wait_send()
    for k in range(2):
        d_copy(k).wait_send()

    def sent(q, carry):
        for j in range(4):
            if j == 0:

                @pl.when(jnp.logical_not((q == 0) & is_self))
                def _():
                    dispatch_copy(q, j).wait_send()

                @pl.when(jnp.logical_not((q == m_own) & is_self))
                def _():
                    return_copy(j, q).wait_send()
            else:
                dispatch_copy(q, j).wait_send()
                return_copy(j, q).wait_send()
        return carry

    lax.fori_loop(0, NQ, sent, 0)


def body(
    tokens, norm_gain, routing, route_weight, w_gate, w_up, w_down, w_branch_in, w_branch_out, branch_gate
):
    bf16, f32 = jnp.bfloat16, jnp.float32
    vmem = pl.BlockSpec(memory_space=pltpu.VMEM)
    hbm = pl.BlockSpec(memory_space=pl.ANY)
    dma = pltpu.SemaphoreType.DMA
    bw = jnp.stack([w_branch_in, w_branch_out.T])
    return pl.pallas_call(
        kernel,
        out_shape=jax.ShapeDtypeStruct((T, F), bf16),
        in_specs=[hbm, hbm, vmem, vmem, vmem, hbm, hbm, hbm, hbm, vmem],
        out_specs=vmem,
        scratch_shapes=[
            pltpu.VMEM((T, F), bf16),
            pltpu.VMEM((4, 8, F), f32),
            pltpu.VMEM((NQ, BLK, F), bf16),
            pltpu.VMEM((NQ, CAP, 4 * F), bf16),
            pltpu.VMEM((3, 4, 512, 512), bf16),
            pltpu.VMEM((2, 8, 4, 2, 32, 1024), bf16),
            pltpu.VMEM((BLK, 4 * F), bf16),
            pltpu.VMEM((BLK, 512), bf16),
            pltpu.VMEM((4, NQ, CAP, F), bf16),
            pltpu.VMEM((64, CAP, F), bf16),
            pltpu.VMEM((192, 4 * F), bf16),
            pltpu.VMEM((192, 4 * F), bf16),
            pltpu.VMEM((192, 1024), bf16),
            pltpu.VMEM((4, 192, F), bf16),
            pltpu.VMEM((T, F), bf16),
            pltpu.VMEM((T, F), f32),
            dma((7,)),
            dma((4,)), dma((4,)),
            dma((4,)), dma((4,)),
            dma((4,)), dma((4,)),
            dma((8,)), dma((8,)),
            dma((2, 4)), dma((2, 4)),
            dma((3, 2)), dma((3, 2)),
            dma((2,)), dma((2,)),
            dma((3, 2)), dma((3, 2)),
            dma((2, 2)), dma((2, 2)),
            dma((64,)), dma((64,)),
            dma((64,)), dma((64,)),
        ],
        compiler_params=pltpu.CompilerParams(has_side_effects=True, vmem_limit_bytes=60 * 1024 * 1024),
        name="layer",
    )(
        tokens,
        jnp.broadcast_to(norm_gain[None, :], (8, F)),
        routing.T,
        routing,
        route_weight,
        w_gate[0],
        w_up[0],
        w_down[0],
        bw,
        jnp.broadcast_to(branch_gate[None, :], (8, F)),
    )


def solution(mesh):
    return jax.shard_map(
        body,
        mesh=mesh,
        in_specs=(
            P("ep", "tp"),
            P("tp"),
            P("ep", None),
            P("ep", None),
            P("ep", "tp", None),
            P("ep", "tp", None),
            P("ep", None, "tp"),
            P("ep", "tp"),
            P("tp", "ep"),
            P("tp"),
        ),
        out_specs=P("ep", "tp"),
        check_vma=False,
    )
```

```python
import functools

import jax
import jax.numpy as jnp
from jax import lax
from jax.experimental import pallas as pl
from jax.experimental.pallas import tpu as pltpu
from jax.sharding import PartitionSpec as P

EPSILON = 1e-06
MESH = pl.DeviceIdType.MESH
CAP = 48
F = 512
T = 768
NQ = 16
BLK = 4 * CAP
EARLY = 14
FIRST = 4


def kernel(
    tok_hbm, gain_hbm, rout_t, rw_t, wg_hbm, wu_hbm, wd_hbm, bwi_hbm, bwo_hbm, gate_ref,
    out_ref,
    tok, gains, send, land, weights, bw, normed, hidden, result, ret, btok, bnorm, bhid, bres, bret, acc, slots_v,
    lsem, gsend, grecv, btsend, btrecv, brsend, brrecv, zsend, zrecv, xsend, xrecv, ysend, yrecv, dsend, drecv,
    wsend, wrecv, fsend, csend, esend, erecv, rsend, rrecv,
):
    ep = lax.axis_index("ep")
    x = lax.axis_index("tp")
    z, y, c = ep // 8, (ep // 2) % 4, ep % 2
    m_own, s4 = ep // 4, ep % 4
    served = (ep // 2) * 2 + x // 2
    sigma = ((x % 2) * 2 + c - served % 4 + 4) % 4
    is_self = sigma == s4
    primary = x // 2 == c
    rel = (x - 2 * c + 4) % 4

    def remote(src, dst, ssem, rsem, e, xx):
        return pltpu.make_async_remote_copy(
            src_ref=src, dst_ref=dst, send_sem=ssem, recv_sem=rsem,
            device_id={"ep": e, "tp": xx}, device_id_type=MESH,
        )

    def lanes(index, width):
        return pl.ds(pl.multiple_of(index * width, width), width)

    def ep_of(zz, yy, cc):
        return (zz * 4 + yy) * 2 + cc

    def block_at(q):
        half = (q + 1) // 2
        return (m_own + 16 + half * (2 * (q % 2) - 1)) % 16

    def target_of(m, j):
        xx = (x + j) % 4
        h = 2 * (xx % 2) + (s4 + xx // 2) % 2
        r = (h - s4 + 4) % 4
        return r, m * 4 + 2 * (r // 2) + h % 2, xx

    barrier = pltpu.get_barrier_semaphore()

    def greet_one(e, xx):
        pl.semaphore_signal(barrier, inc=1, device_id={"ep": e, "tp": xx}, device_id_type=MESH)

    for d in range(1, 8):
        greet_one(ep_of((z + d) % 8, y, c), x)
    for d in range(1, 4):
        greet_one(ep, (x + d) % 4)
    for d in (1, 3):
        greet_one(ep_of(z, (y + d) % 4, c), x)
    greet_one(ep_of(z, y, 1 - c), x)

    def greet(m, carry):
        for j in range(4):
            _, e, xx = target_of(m, j)

            @pl.when(jnp.logical_not((e == ep) & (xx == x)))
            def _():
                greet_one(e, xx)

            @pl.when(jnp.logical_not(is_self & (m == m_own) & (j == 0)))
            def _():
                greet_one(m * 4 + sigma, xx)
        return carry

    lax.fori_loop(0, NQ, greet, 0)

    loads = [
        pltpu.make_async_copy(tok_hbm, tok, lsem.at[0]),
        pltpu.make_async_copy(bwi_hbm, bw.at[0, z, y, c, :, lanes(x, 256)], lsem.at[1]),
        pltpu.make_async_copy(bwo_hbm, bw.at[1, z, y, c, :, lanes(x, 256)], lsem.at[2]),
        pltpu.make_async_copy(gain_hbm, gains.at[x], lsem.at[3]),
        pltpu.make_async_copy(tok_hbm.at[pl.ds(x * 192, 192), :], btok.at[:, lanes(x, F)], lsem.at[4]),
    ]
    for load in loads:
        load.start()
    w_hbm = (wg_hbm, wu_hbm, wd_hbm)
    w_loads = [pltpu.make_async_copy(w_hbm[k], weights.at[k, x], lsem.at[5 + k]) for k in range(3)]

    @pl.when(primary)
    def _():
        for load in w_loads:
            load.start()

    experts = lax.broadcasted_iota(jnp.int32, (64, T), 0)
    r0, r1 = rout_t[0:1, :], rout_t[1:2, :]
    named0, named1 = experts == r0, experts == r1
    one_hot = jnp.where(named0 | named1, 1.0, 0.0).astype(jnp.bfloat16)
    earlier = jnp.where(
        lax.broadcasted_iota(jnp.int32, (T, T), 0) < lax.broadcasted_iota(jnp.int32, (T, T), 1), 1.0, 0.0
    ).astype(jnp.bfloat16)
    before = jnp.dot(one_hot, earlier, preferred_element_type=jnp.float32)
    slot0 = r0 * CAP + jnp.sum(jnp.where(named0, before, 0.0), axis=0, keepdims=True).astype(jnp.int32)
    slot1 = r1 * CAP + jnp.sum(jnp.where(named1, before, 0.0), axis=0, keepdims=True).astype(jnp.int32)
    slots_v[0:1, :] = slot0.astype(jnp.float32)
    slots_v[1:2, :] = slot1.astype(jnp.float32)
    slots_v[2:4, :] = rw_t[...]
    slots_v[4:8, :] = jnp.zeros((4, T), jnp.float32)

    for load in loads:
        load.wait()

    def dispatch_copy(q, j):
        m = block_at(q)
        r, e, xx = target_of(m, j)
        return remote(
            send.at[m, pl.ds(pl.multiple_of(r * CAP, 16), CAP), :],
            land.at[m_own, :, lanes(x, F)],
            esend.at[q * 4 + j],
            erecv.at[m_own * 4 + x],
            e,
            xx,
        )

    def pack(q, carry):
        m = block_at(q)
        slots = lax.broadcasted_iota(jnp.int32, (BLK, T), 0) + m * BLK
        pick = jnp.where((slots == slot0) | (slots == slot1), 1.0, 0.0).astype(jnp.bfloat16)
        send[m] = jnp.dot(pick, tok[...], preferred_element_type=jnp.float32).astype(jnp.bfloat16)
        return carry

    def dispatch(q, carry):
        for j in range(4):
            if j == 0:
                own = (q == 0) & is_self

                @pl.when(jnp.logical_not(own))
                def _():
                    dispatch_copy(q, j).start()

                @pl.when(own)
                def _():
                    r, _, _ = target_of(m_own, 0)
                    land[m_own, :, lanes(x, F)] = send[m_own, pl.ds(pl.multiple_of(r * CAP, 16), CAP), :]
            else:
                dispatch_copy(q, j).start()
        return carry

    def pack_and_send(q, carry):
        return dispatch(q, pack(q, carry))

    lax.fori_loop(0, EARLY, pack, 0)
    pl.semaphore_wait(barrier, 13 + 128 - 2 * is_self.astype(jnp.int32))

    mate = (x + 5 - 2 * rel) % 4
    outer = (x + 3 + 2 * rel) % 4
    inner = (x + 2 * rel + 3) % 4

    def w_own(k, to):
        return remote(w_hbm[k], weights.at[k, x], wsend.at[k], wrecv.at[k, x], ep, to)

    def w_piece(k, slot, sem, e, to):
        return remote(weights.at[k, slot], weights.at[k, slot], sem, wrecv.at[k, slot], e, to)

    def w_forward(k):
        return w_piece(k, outer, fsend.at[k], ep, mate)

    def w_across(k, slot):
        return w_piece(k, slot, csend.at[k, slot], ep_of(z, y, 1 - c), x)

    def w_start(ks):
        @pl.when(primary)
        def _():
            for k in ks:
                w_own(k, mate).start()

        @pl.when(jnp.logical_not(primary))
        def _():
            for k in ks:
                w_own(k, inner).start()

    def z_copy(d):
        zz = (z + d) % 8
        mine = bw.at[:, z, y, c, :, lanes(x, 256)]
        return remote(mine, mine, zsend.at[d], zrecv.at[d], ep_of(zz, y, c), x)

    def x_copy(k, d):
        mine = bw.at[k, :, y, c, :, lanes(x, 256)]
        return remote(mine, mine, xsend.at[k, d], xrecv.at[k, d], ep, (x + d) % 4)

    def y_copy(k, way):
        mine = bw.at[k, :, y, c]
        return remote(mine, mine, ysend.at[k, way], yrecv.at[k, way], ep_of(z, (y + (1, 3)[way]) % 4, c), x)

    def y_forward(way):
        slot = (y + (3, 1)[way]) % 4
        piece = bw.at[way, :, slot, c]
        return remote(piece, piece, ysend.at[2, way], yrecv.at[2, way], ep_of(z, (y + (1, 3)[way]) % 4, c), x)

    def d_copy(k):
        mine = bw.at[k, :, :, c]
        return remote(mine, mine, dsend.at[k], drecv.at[k], ep_of(z, y, 1 - c), x)

    def gain_copy(d):
        return remote(gains.at[x], gains.at[x], gsend.at[d], grecv.at[d], ep, (x + d) % 4)

    def btok_copy(d):
        xx = (x + d) % 4
        return remote(
            tok.at[pl.ds(xx * 192, 192), :], btok.at[:, lanes(x, F)], btsend.at[d], btrecv.at[d], ep, xx
        )

    for d in range(1, 8):
        z_copy(d).start()
    for d in range(1, 4):
        gain_copy(d).start()
    w_start((0, 1, 2))
    lax.fori_loop(0, FIRST, dispatch, 0)

    @pl.when(primary)
    def _():
        for k in range(3):
            w_loads[k].wait()
            w_across(k, x).start()

    for d in range(1, 8):
        z_copy(d).wait_recv()
    for d in range(1, 4):
        for k in range(2):
            x_copy(k, d).start()
    lax.fori_loop(FIRST, EARLY, dispatch, 0)
    lax.fori_loop(EARLY, NQ, pack_and_send, 0)

    @pl.when(primary)
    def _():
        for k in range(3):
            w_piece(k, outer, fsend.at[k], ep, x).wait_recv()
            w_forward(k).start()
            w_across(k, outer).start()
            w_piece(k, mate, fsend.at[k], ep, x).wait_recv()
            w_across(k, mate).start()

    for d in range(1, 4):
        for k in range(2):
            x_copy(k, d).wait_recv()
    for way in range(2):
        for k in range(2):
            y_copy(k, way).start()
    for d in range(1, 4):
        btok_copy(d).start()

    @pl.when(primary)
    def _():
        for k in range(3):
            w_piece(k, (x + 2) % 4, fsend.at[k], ep, x).wait_recv()
            w_across(k, (x + 2) % 4).start()

    for d in range(1, 4):
        gain_copy(d).wait_recv()

    @pl.when(jnp.logical_not(primary))
    def _():
        for k in range(3):
            for h in range(4):
                w_piece(k, h, fsend.at[k], ep, x).wait_recv()

    for way in range(2):
        for k in range(2):
            y_copy(k, way).wait_recv()
    for way in range(2):
        y_forward(way).start()

    def norm_rows(source, target):
        floats = source.astype(jnp.float32)
        squares = jnp.sum(floats * floats, axis=1, keepdims=True)
        scaled = floats * lax.rsqrt(squares * (1.0 / (4 * F)) + EPSILON)
        for k in range(4):
            target[:, k * F : (k + 1) * F] = (scaled[:, k * F : (k + 1) * F] * gains[k]).astype(jnp.bfloat16)

    def arrival(m, xx):
        there = land.at[m, :, lanes(xx, F)]
        return remote(there, there, esend.at[0], erecv.at[m * 4 + xx], ep, xx)

    def return_copy(jj, m):
        quarter = (x + (0, 1, 3, 2)[jj]) % 4
        return remote(
            result.at[quarter, m], ret.at[served], rsend.at[jj * 16 + m], rrecv.at[served], m * 4 + sigma, quarter
        )

    def expert(i, carry):
        part = (z // 2 + i) % 4
        for mm in range(4):
            m = part * 4 + mm
            for xx in range(4):

                @pl.when(jnp.logical_not(is_self & (m == m_own) & (x == xx)))
                def _():
                    arrival(m, xx).wait_recv()

        def one(r, inner):
            m, row = part * 4 + r // 3, pl.multiple_of((r % 3) * 16, 16)
            norm_rows(land[m, pl.ds(row, 16), :], normed.at[pl.ds(pl.multiple_of(r * 16, 16), 16), :])
            return inner

        lax.fori_loop(0, 12, one, 0)
        for n in range(2):
            cols = slice(n * 256, n * 256 + 256)
            sums = []
            for k in range(2):
                total = jnp.dot(normed[:, 0:F], weights[k, 0, :, cols], preferred_element_type=jnp.float32)
                for h in range(1, 4):
                    total += jnp.dot(
                        normed[:, h * F : (h + 1) * F], weights[k, h, :, cols], preferred_element_type=jnp.float32
                    )
                sums.append(total)
            gate_sum, up_sum = sums
            hidden[:, cols] = (gate_sum / (1.0 + jnp.exp(-gate_sum)) * up_sum).astype(jnp.bfloat16)
        for jj in range(4):
            quarter = (x + (0, 1, 3, 2)[jj]) % 4
            rows = jnp.dot(hidden[...], weights[2, quarter], preferred_element_type=jnp.float32)
            result[quarter, pl.ds(part * 4, 4)] = rows.astype(jnp.bfloat16).reshape(4, CAP, F)
            for mm in range(4):
                m = part * 4 + mm
                if jj == 0:
                    own = is_self & (m == m_own)

                    @pl.when(jnp.logical_not(own))
                    def _():
                        return_copy(jj, m).start()

                    @pl.when(own)
                    def _():
                        ret[served] = result[x, m_own]
                else:
                    return_copy(jj, m).start()

        @pl.when(i == 2)
        def _():
            for way in range(2):
                y_forward(way).wait_recv()
            for k in range(2):
                d_copy(k).start()

        return carry

    lax.fori_loop(0, 4, expert, 0)

    for d in range(1, 4):
        btok_copy(d).wait_recv()

    def branch_norm(r, carry):
        rows = pl.ds(pl.multiple_of(r * 16, 16), 16)
        norm_rows(btok[rows, :], bnorm.at[rows, :])
        return carry

    lax.fori_loop(0, 12, branch_norm, 0)

    columns = slots_v[...].T
    place0, place1, rw0, rw1 = (columns[:, k : k + 1] for k in range(4))

    for k in range(2):
        d_copy(k).wait_recv()

    w_in = bw.at[0].reshape(2048, 1024)
    w_out = bw.at[1].reshape(2048, 1024)
    for n in range(4):
        cols = slice(n * 256, n * 256 + 256)
        total = jnp.dot(bnorm[...], w_in[:, cols], preferred_element_type=jnp.float32)
        bhid[:, cols] = (total / (1.0 + jnp.exp(-total))).astype(jnp.bfloat16)

    def bret_copy(d):
        xx = (x + d) % 4
        return remote(
            bres.at[xx], bret.at[pl.ds(x * 192, 192), :], brsend.at[d], brrecv.at[d], ep, xx
        )

    for d in (1, 3, 2, 0):
        quarter = (x + d) % 4
        rows = lax.dot_general(
            bhid[...],
            w_out[pl.ds(pl.multiple_of(quarter * F, F), F), :],
            (((1,), (1,)), ((), ())),
            preferred_element_type=jnp.float32,
        )
        if d == 0:
            bret[pl.ds(pl.multiple_of(x * 192, 192), 192), :] = rows.astype(jnp.bfloat16)
        else:
            bres[quarter] = rows.astype(jnp.bfloat16)
            bret_copy(d).start()

    for d in range(1, 8):
        z_copy(d).wait_send()
    for d in range(1, 4):
        gain_copy(d).wait_send()
        btok_copy(d).wait_send()
        for k in range(2):
            x_copy(k, d).wait_send()
    for way in range(2):
        for k in range(2):
            y_copy(k, way).wait_send()
        y_forward(way).wait_send()
    for k in range(2):
        d_copy(k).wait_send()
    for k in range(3):
        w_own(k, x).wait_send()

    @pl.when(primary)
    def _():
        for k in range(3):
            w_forward(k).wait_send()
            for h in range(4):
                w_across(k, h).wait_send()

    def dispatched(q, carry):
        for j in range(4):
            if j == 0:

                @pl.when(jnp.logical_not((q == 0) & is_self))
                def _():
                    dispatch_copy(q, j).wait_send()
            else:
                dispatch_copy(q, j).wait_send()
        return carry

    lax.fori_loop(0, NQ, dispatched, 0)

    acc[...] = jnp.zeros_like(acc)

    def returned(e):
        return remote(ret.at[e], ret.at[e], rsend.at[0], rrecv.at[e], ep, x)

    def combine(i, carry):
        part = (z // 2 + i) % 4

        def wait(k, inner):
            e = part * 16 + k

            @pl.when(jnp.logical_not(is_self & (e == served)))
            def _():
                returned(e).wait_recv()

            return inner

        lax.fori_loop(0, 16, wait, 0)
        rows = ret[pl.ds(part * 16, 16)].reshape(16 * CAP, F)
        for h in range(3):
            sl = slice(h * 256, h * 256 + 256)
            slots = (lax.broadcasted_iota(jnp.int32, (256, 16 * CAP), 1) + part * (16 * CAP)).astype(jnp.float32)
            mix = jnp.where(slots == place0[sl], rw0[sl], 0.0) + jnp.where(slots == place1[sl], rw1[sl], 0.0)
            acc[sl, :] += jnp.dot(mix.astype(jnp.bfloat16), rows, preferred_element_type=jnp.float32)
        return carry

    lax.fori_loop(0, 4, combine, 0)
    for d in range(1, 4):
        bret_copy(d).wait_recv()
    share = 1.0 / (1.0 + jnp.exp(-gate_ref[0:1, :]))
    for h in range(3):
        sl = slice(h * 256, h * 256 + 256)
        out_ref[sl, :] = (acc[sl, :] + share * bret[sl, :].astype(jnp.float32)).astype(jnp.bfloat16)

    for d in range(1, 4):
        bret_copy(d).wait_send()

    def sent(q, carry):
        for j in range(4):
            if j == 0:

                @pl.when(jnp.logical_not((q == m_own) & is_self))
                def _():
                    return_copy(j, q).wait_send()
            else:
                return_copy(j, q).wait_send()
        return carry

    lax.fori_loop(0, NQ, sent, 0)


def body(
    tokens, norm_gain, routing, route_weight, w_gate, w_up, w_down, w_branch_in, w_branch_out, branch_gate
):
    bf16, f32 = jnp.bfloat16, jnp.float32
    vmem = pl.BlockSpec(memory_space=pltpu.VMEM)
    hbm = pl.BlockSpec(memory_space=pl.ANY)
    dma = pltpu.SemaphoreType.DMA
    return pl.pallas_call(
        kernel,
        out_shape=jax.ShapeDtypeStruct((T, F), bf16),
        in_specs=[hbm, hbm, vmem, vmem, hbm, hbm, hbm, hbm, hbm, vmem],
        out_specs=vmem,
        scratch_shapes=[
            pltpu.VMEM((T, F), bf16),
            pltpu.VMEM((4, 1, F), f32),
            pltpu.VMEM((NQ, BLK, F), bf16),
            pltpu.VMEM((NQ, CAP, 4 * F), bf16),
            pltpu.VMEM((3, 4, 512, 512), bf16),
            pltpu.VMEM((2, 8, 4, 2, 32, 1024), bf16),
            pltpu.VMEM((BLK, 4 * F), bf16),
            pltpu.VMEM((BLK, 512), bf16),
            pltpu.VMEM((4, NQ, CAP, F), bf16),
            pltpu.VMEM((64, CAP, F), bf16),
            pltpu.VMEM((192, 4 * F), bf16),
            pltpu.VMEM((192, 4 * F), bf16),
            pltpu.VMEM((192, 1024), bf16),
            pltpu.VMEM((4, 192, F), bf16),
            pltpu.VMEM((T, F), bf16),
            pltpu.VMEM((T, F), f32),
            pltpu.VMEM((8, T), f32),
            dma((8,)),
            dma((4,)), dma((4,)),
            dma((4,)), dma((4,)),
            dma((4,)), dma((4,)),
            dma((8,)), dma((8,)),
            dma((2, 4)), dma((2, 4)),
            dma((3, 2)), dma((3, 2)),
            dma((2,)), dma((2,)),
            dma((3,)), dma((3, 4)),
            dma((3,)), dma((3, 4)),
            dma((64,)), dma((64,)),
            dma((64,)), dma((64,)),
        ],
        compiler_params=pltpu.CompilerParams(collective_id=0, has_side_effects=True, vmem_limit_bytes=60 * 1024 * 1024),
        name="layer",
    )(
        tokens,
        norm_gain.reshape(1, F),
        routing.T,
        route_weight.T,
        w_gate[0],
        w_up[0],
        w_down[0],
        w_branch_in,
        w_branch_out.T,
        branch_gate.reshape(1, F),
    )


def solution(mesh):
    return jax.shard_map(
        body,
        mesh=mesh,
        in_specs=(
            P("ep", "tp"),
            P("tp"),
            P("ep", None),
            P("ep", None),
            P("ep", "tp", None),
            P("ep", "tp", None),
            P("ep", None, "tp"),
            P("ep", "tp"),
            P("tp", "ep"),
            P("tp"),
        ),
        out_specs=P("ep", "tp"),
        check_vma=False,
    )
```

```python
import jax
import jax.numpy as jnp
from jax import lax
from jax.experimental import pallas as pl
from jax.experimental.pallas import tpu as pltpu
from jax.sharding import PartitionSpec as P

EPSILON = 1e-06
MESH = pl.DeviceIdType.MESH
CAP = 48
F = 512
T = 768
NQ = 16
BLK = 4 * CAP
GT = 384
MEM = 16
FIRST, SECOND = 3, 6


def kernel(
    tok_hbm, gain_hbm, rout_t, rw_t, wg_hbm, wu_hbm, wd_hbm, bwi_hbm, bwo_hbm, gate_ref,
    out_ref,
    tok, gains, send, land, weights, bw, normed, hidden, result, rr, btok, bnorm, bhid, bres, bret, acc, gslot_v,
    meta_out, meta, mix, rq, back,
    lsem, gsend, grecv, btsend, btrecv, brsend, brrecv, zsend, zrecv, xsend, xrecv, ysend, yrecv, dsend, drecv,
    wsend, wrecv, fsend, csend, esend, erecv, rsend, rrecv, msend, mrecv, s4send, s4recv,
):
    ep = lax.axis_index("ep")
    x = lax.axis_index("tp")
    z, y, c = ep // 8, (ep // 2) % 4, ep % 2
    m_own, s4 = ep // 4, ep % 4
    served = (ep // 2) * 2 + x // 2
    sigma = ((x % 2) * 2 + c - served % 4 + 4) % 4
    is_self = sigma == s4
    primary = x // 2 == c
    rel = (x - 2 * c + 4) % 4

    def remote(src, dst, ssem, rsem, e, xx):
        return pltpu.make_async_remote_copy(
            src_ref=src, dst_ref=dst, send_sem=ssem, recv_sem=rsem,
            device_id={"ep": e, "tp": xx}, device_id_type=MESH,
        )

    def lanes(index, width):
        return pl.ds(pl.multiple_of(index * width, width), width)

    def ep_of(zz, yy, cc):
        return (zz * 4 + yy) * 2 + cc

    def block_at(q):
        half = (q + 1) // 2
        return (m_own + 16 + half * (2 * (q % 2) - 1)) % 16

    def target_of(m, j):
        xx = (x + j) % 4
        h = 2 * (xx % 2) + (s4 + xx // 2) % 2
        r = (h - s4 + 4) % 4
        return r, m * 4 + 2 * (r // 2) + h % 2, xx

    group, mine_in = z // 2, served % MEM

    def relay_of(zz, g):
        ahead = (2 * g - zz + 16) % 8
        return jnp.where(ahead <= 3, 2 * g, 2 * g + 1), jnp.where(ahead <= 3, ahead, 7 - ahead)

    def source_z(k):
        return jnp.where(z % 2 == 0, z - k + 8, z + k) % 8

    barrier = pltpu.get_barrier_semaphore()

    def greet_one(e, xx):
        pl.semaphore_signal(barrier, inc=1, device_id={"ep": e, "tp": xx}, device_id_type=MESH)

    for d in range(1, 8):
        greet_one(ep_of((z + d) % 8, y, c), x)
    for d in range(1, 4):
        greet_one(ep, (x + d) % 4)
        greet_one(ep_of(source_z(d), y, c), x)
        greet_one(ep_of(relay_of(z, (group + d) % 4)[0], y, c), x)
    for d in (1, 3):
        greet_one(ep_of(z, (y + d) % 4, c), x)
    greet_one(ep_of(z, y, 1 - c), x)

    def greet(m, carry):
        for j in range(4):

            @pl.when(jnp.logical_not(is_self & (m == m_own) & (j == 0)))
            def _():
                greet_one(m * 4 + sigma, (x + j) % 4)

        @pl.when(jnp.logical_not(is_self & (m == mine_in)))
        def _():
            h = (s4 + m) % 4
            greet_one(group * MEM + (m // 2) * 2 + h % 2, 2 * (m % 2) + h // 2)

        return carry

    lax.fori_loop(0, NQ, greet, 0)

    loads = [
        pltpu.make_async_copy(tok_hbm, tok, lsem.at[0]),
        pltpu.make_async_copy(bwi_hbm, bw.at[0, z, y, c, :, lanes(x, 256)], lsem.at[1]),
        pltpu.make_async_copy(bwo_hbm, bw.at[1, z, y, c, :, lanes(x, 256)], lsem.at[2]),
        pltpu.make_async_copy(gain_hbm, gains.at[x], lsem.at[3]),
        pltpu.make_async_copy(tok_hbm.at[pl.ds(x * 192, 192), :], btok.at[:, lanes(x, F)], lsem.at[4]),
    ]
    for load in loads:
        load.start()
    w_hbm = (wg_hbm, wu_hbm, wd_hbm)
    w_loads = [pltpu.make_async_copy(w_hbm[k], weights.at[k, x], lsem.at[5 + k]) for k in range(3)]

    @pl.when(primary)
    def _():
        for load in w_loads:
            load.start()

    experts = lax.broadcasted_iota(jnp.int32, (64, T), 0)
    r0, r1 = rout_t[0:1, :], rout_t[1:2, :]
    named0, named1 = experts == r0, experts == r1
    gid = r0 // MEM
    in_group = lax.broadcasted_iota(jnp.int32, (16, T), 0) == gid
    one_hot = jnp.concatenate(
        [
            jnp.where(named0 | named1, 1.0, 0.0).astype(jnp.bfloat16),
            jnp.where(in_group, 1.0, 0.0).astype(jnp.bfloat16),
        ],
        axis=0,
    )
    earlier = jnp.where(
        lax.broadcasted_iota(jnp.int32, (T, T), 0) < lax.broadcasted_iota(jnp.int32, (T, T), 1), 1.0, 0.0
    ).astype(jnp.bfloat16)
    before = jnp.dot(one_hot, earlier, preferred_element_type=jnp.float32)
    pos0 = jnp.sum(jnp.where(named0, before[:64], 0.0), axis=0, keepdims=True)
    pos1 = jnp.sum(jnp.where(named1, before[:64], 0.0), axis=0, keepdims=True)
    rank = jnp.sum(jnp.where(in_group, before[64:], 0.0), axis=0, keepdims=True)
    slot0 = r0 * CAP + pos0.astype(jnp.int32)
    slot1 = r1 * CAP + pos1.astype(jnp.int32)
    gslot = (gid * GT).astype(jnp.float32) + rank
    gslot_v[...] = jnp.broadcast_to(gslot, (8, T))
    facts = jnp.concatenate(
        [
            (r0 - gid * MEM).astype(jnp.float32),
            pos0,
            (r1 - gid * MEM).astype(jnp.float32),
            pos1,
            rw_t[...],
            jnp.zeros((2, T), jnp.float32),
        ],
        axis=0,
    ).astype(jnp.bfloat16)

    for load in loads:
        load.wait()

    def dispatch_copy(q, j):
        m = block_at(q)
        r, e, xx = target_of(m, j)
        return remote(
            send.at[m, pl.ds(pl.multiple_of(r * CAP, 16), CAP), :],
            land.at[m_own, :, lanes(x, F)],
            esend.at[q * 4 + j],
            erecv.at[m_own * 4 + x],
            e,
            xx,
        )

    def pack(q, carry):
        m = block_at(q)
        slots = lax.broadcasted_iota(jnp.int32, (BLK, T), 0) + m * BLK
        pick = jnp.where((slots == slot0) | (slots == slot1), 1.0, 0.0).astype(jnp.bfloat16)
        send[m] = jnp.dot(pick, tok[...], preferred_element_type=jnp.float32).astype(jnp.bfloat16)
        return carry

    def dispatch_straight(q, carry):
        own = (q == 0) & is_self

        @pl.when(jnp.logical_not(own))
        def _():
            dispatch_copy(q, 0).start()

        @pl.when(own)
        def _():
            r, _, _ = target_of(m_own, 0)
            land[m_own, :, lanes(x, F)] = send[m_own, pl.ds(pl.multiple_of(r * CAP, 16), CAP), :]

        return carry

    def dispatch_across(q, carry):
        for j in range(1, 4):
            dispatch_copy(q, j).start()
        return carry

    lax.fori_loop(0, NQ, pack, 0)
    pl.semaphore_wait(barrier, 13 + 6 + 64 + 16 - 2 * is_self.astype(jnp.int32))

    mate = (x + 5 - 2 * rel) % 4
    outer = (x + 3 + 2 * rel) % 4
    inner = (x + 2 * rel + 3) % 4

    def w_own(k, to):
        return remote(w_hbm[k], weights.at[k, x], wsend.at[k], wrecv.at[k, x], ep, to)

    def w_piece(k, slot, sem, e, to):
        return remote(weights.at[k, slot], weights.at[k, slot], sem, wrecv.at[k, slot], e, to)

    def w_forward(k):
        return w_piece(k, outer, fsend.at[k], ep, mate)

    def w_across(k, slot):
        return w_piece(k, slot, csend.at[k, slot], ep_of(z, y, 1 - c), x)

    def w_start(ks):
        @pl.when(primary)
        def _():
            for k in ks:
                w_own(k, mate).start()

        @pl.when(jnp.logical_not(primary))
        def _():
            for k in ks:
                w_own(k, inner).start()

    def z_copy(d):
        zz = (z + d) % 8
        mine = bw.at[:, z, y, c, :, lanes(x, 256)]
        return remote(mine, mine, zsend.at[d], zrecv.at[d], ep_of(zz, y, c), x)

    def x_copy(k, d):
        mine = bw.at[k, :, y, c, :, lanes(x, 256)]
        return remote(mine, mine, xsend.at[k, d], xrecv.at[k, d], ep, (x + d) % 4)

    def y_copy(k, way):
        mine = bw.at[k, :, y, c]
        return remote(mine, mine, ysend.at[k, way], yrecv.at[k, way], ep_of(z, (y + (1, 3)[way]) % 4, c), x)

    def y_forward(way):
        slot = (y + (3, 1)[way]) % 4
        piece = bw.at[way, :, slot, c]
        return remote(piece, piece, ysend.at[2, way], yrecv.at[2, way], ep_of(z, (y + (1, 3)[way]) % 4, c), x)

    def d_copy(k):
        mine = bw.at[k, :, :, c]
        return remote(mine, mine, dsend.at[k], drecv.at[k], ep_of(z, y, 1 - c), x)

    def gain_copy(d):
        return remote(gains.at[x], gains.at[x], gsend.at[d], grecv.at[d], ep, (x + d) % 4)

    def btok_copy(d):
        xx = (x + d) % 4
        return remote(
            tok.at[pl.ds(xx * 192, 192), :], btok.at[:, lanes(x, F)], btsend.at[d], btrecv.at[d], ep, xx
        )

    for d in range(1, 8):
        z_copy(d).start()
    for d in range(1, 4):
        gain_copy(d).start()
    w_start((0, 1))
    lax.fori_loop(0, NQ, dispatch_straight, 0)

    @pl.when(primary)
    def _():
        for k in range(3):
            w_loads[k].wait()
            w_across(k, x).start()

    def w_relay(k):
        w_piece(k, outer, fsend.at[k], ep, x).wait_recv()
        w_forward(k).start()
        w_across(k, outer).start()
        w_piece(k, mate, fsend.at[k], ep, x).wait_recv()
        w_across(k, mate).start()

    def w_last(k):
        w_piece(k, (x + 2) % 4, fsend.at[k], ep, x).wait_recv()
        w_across(k, (x + 2) % 4).start()

    def w_served(k):
        for h in range(4):
            w_piece(k, h, fsend.at[k], ep, x).wait_recv()

    for d in range(1, 8):
        z_copy(d).wait_recv()
    for d in range(1, 4):
        for k in range(2):
            x_copy(k, d).start()

    lax.fori_loop(0, FIRST, dispatch_across, 0)

    def m_copy(d):
        g = (group + d) % 4
        plane, k = relay_of(z, g)
        return remote(meta_out.at[g], meta.at[k], msend.at[d], mrecv.at[k], ep_of(plane, y, c), x)

    for d in range(4):
        g = (group + d) % 4
        places = (lax.broadcasted_iota(jnp.int32, (GT, T), 0) + g * GT).astype(jnp.float32)
        pick = jnp.where(places == gslot, 1.0, 0.0).astype(jnp.bfloat16)
        told = lax.dot_general(facts, pick, (((1,), (1,)), ((), ())), preferred_element_type=jnp.float32)
        if d == 0:
            meta[0] = told
        else:
            meta_out[g] = told
            m_copy(d).start()


    @pl.when(primary)
    def _():
        for k in range(2):
            w_relay(k)

    lax.fori_loop(FIRST, SECOND, dispatch_across, 0)
    for d in range(1, 4):
        for k in range(2):
            x_copy(k, d).wait_recv()
    for way in range(2):
        for k in range(2):
            y_copy(k, way).start()
    lax.fori_loop(SECOND, NQ, dispatch_across, 0)
    w_start((2,))

    for k in range(1, 4):
        remote(meta.at[k], meta.at[k], msend.at[0], mrecv.at[k], ep, x).wait_recv()
    for k in range(4):
        columns = meta[k].T
        at0 = columns[:, 0:1] * CAP + columns[:, 1:2]
        at1 = columns[:, 2:3] * CAP + columns[:, 3:4]
        for h in range(2):
            sl = slice(h * 192, h * 192 + 192)
            slots = lax.broadcasted_iota(jnp.int32, (192, T), 1).astype(jnp.float32)
            mix[k, sl, :] = (
                jnp.where(slots == at0[sl], columns[sl, 4:5], 0.0)
                + jnp.where(slots == at1[sl], columns[sl, 5:6], 0.0)
            ).astype(jnp.bfloat16)

    @pl.when(primary)
    def _():
        w_relay(2)

    for way in range(2):
        for k in range(2):
            y_copy(k, way).wait_recv()
    for way in range(2):
        y_forward(way).start()

    @pl.when(primary)
    def _():
        for k in range(2):
            w_last(k)

    for d in range(1, 4):
        gain_copy(d).wait_recv()

    @pl.when(jnp.logical_not(primary))
    def _():
        for k in range(2):
            w_served(k)

    def norm_rows(source, target):
        floats = source.astype(jnp.float32)
        squares = jnp.sum(floats * floats, axis=1, keepdims=True)
        scaled = floats * lax.rsqrt(squares * (1.0 / (4 * F)) + EPSILON)
        for k in range(4):
            target[:, k * F : (k + 1) * F] = (scaled[:, k * F : (k + 1) * F] * gains[k]).astype(jnp.bfloat16)

    def arrival(m, xx):
        there = land.at[m, :, lanes(xx, F)]
        return remote(there, there, esend.at[0], erecv.at[m * 4 + xx], ep, xx)

    def return_copy(jj, m):
        quarter = (x + (0, 1, 3, 2)[jj]) % 4
        plane, k = relay_of(m // 2, group)
        return remote(
            result.at[quarter, m], rr.at[k, mine_in], rsend.at[jj * 16 + m], rrecv.at[k * MEM + mine_in],
            ep_of(plane, (m % 2) * 2 + sigma // 2, sigma % 2), quarter,
        )

    def stays(m):
        return is_self & (m % 2 == y // 2) & (relay_of(m // 2, group)[0] == z)

    def pair_at(i):
        return jnp.where(i == 0, 2, jnp.where(i == 1, 1, jnp.where(i == 2, 3, 0)))

    def give_back(part, jj):
        for mm in range(4):
            m = part * 4 + mm
            if jj == 0:
                own = stays(m)

                @pl.when(jnp.logical_not(own))
                def _():
                    return_copy(jj, m).start()

                @pl.when(own)
                def _():
                    rr[relay_of(m // 2, group)[1], mine_in] = result[x, m]
            else:
                return_copy(jj, m).start()

    def expert(i, carry):
        part = (z // 2 + pair_at(i)) % 4
        for mm in range(4):
            m = part * 4 + mm
            for xx in range(4):

                @pl.when(jnp.logical_not(is_self & (m == m_own) & (x == xx)))
                def _():
                    arrival(m, xx).wait_recv()

        def one(r, inner):
            m, row = part * 4 + r // 3, pl.multiple_of((r % 3) * 16, 16)
            norm_rows(land[m, pl.ds(row, 16), :], normed.at[pl.ds(pl.multiple_of(r * 16, 16), 16), :])
            return inner

        lax.fori_loop(0, 12, one, 0)
        for n in range(2):
            cols = slice(n * 256, n * 256 + 256)
            sums = []
            for k in range(2):
                total = jnp.dot(normed[:, 0:F], weights[k, 0, :, cols], preferred_element_type=jnp.float32)
                for h in range(1, 4):
                    total += jnp.dot(
                        normed[:, h * F : (h + 1) * F], weights[k, h, :, cols], preferred_element_type=jnp.float32
                    )
                sums.append(total)
            gate_sum, up_sum = sums
            hidden[:, cols] = (gate_sum / (1.0 + jnp.exp(-gate_sum)) * up_sum).astype(jnp.bfloat16)

        @pl.when((i == 0) & primary)
        def _():
            w_last(2)

        @pl.when((i == 0) & jnp.logical_not(primary))
        def _():
            w_served(2)

        for jj in range(4):
            quarter = (x + (0, 1, 3, 2)[jj]) % 4
            rows = jnp.dot(hidden[...], weights[2, quarter], preferred_element_type=jnp.float32)
            result[quarter, pl.ds(part * 4, 4)] = rows.astype(jnp.bfloat16).reshape(4, CAP, F)

            @pl.when(i < 3)
            def _():
                give_back(part, jj)

        return carry

    lax.fori_loop(0, 4, expert, 0)
    for d in range(1, 4):
        btok_copy(d).start()

    def s4_copy(k):
        return remote(rq.at[k], back.at[group], s4send.at[k], s4recv.at[group], ep_of(source_z(k), y, c), x)

    def relay(k):
        def wait(n, inner):
            @pl.when(jnp.logical_not(is_self & (n == mine_in)))
            def _():
                remote(rr.at[k, n], rr.at[k, n], rsend.at[0], rrecv.at[k * MEM + n], ep, x).wait_recv()

            return inner

        lax.fori_loop(0, MEM, wait, 0)
        total = jnp.dot(mix[k], rr[k].reshape(T, F), preferred_element_type=jnp.float32).astype(jnp.bfloat16)
        if k == 0:
            back[group] = total
        else:
            rq[k] = total
            s4_copy(k).start()

    for way in range(2):
        y_forward(way).wait_recv()
    for k in range(2):
        d_copy(k).start()
    relay(3)
    for jj in range(4):
        give_back(group, jj)
    relay(2)
    relay(1)
    for d in range(1, 4):
        btok_copy(d).wait_recv()

    def branch_norm(r, carry):
        rows = pl.ds(pl.multiple_of(r * 16, 16), 16)
        norm_rows(btok[rows, :], bnorm.at[rows, :])
        return carry

    lax.fori_loop(0, 12, branch_norm, 0)

    for k in range(2):
        d_copy(k).wait_recv()

    w_in = bw.at[0].reshape(2048, 1024)
    w_out = bw.at[1].reshape(2048, 1024)
    for n in range(4):
        cols = slice(n * 256, n * 256 + 256)
        total = jnp.dot(bnorm[...], w_in[:, cols], preferred_element_type=jnp.float32)
        bhid[:, cols] = (total / (1.0 + jnp.exp(-total))).astype(jnp.bfloat16)

    def bret_copy(d):
        xx = (x + d) % 4
        return remote(
            bres.at[xx], bret.at[pl.ds(x * 192, 192), :], brsend.at[d], brrecv.at[d], ep, xx
        )

    for d in (1, 3, 2, 0):
        quarter = (x + d) % 4
        rows = lax.dot_general(
            bhid[...],
            w_out[pl.ds(pl.multiple_of(quarter * F, F), F), :],
            (((1,), (1,)), ((), ())),
            preferred_element_type=jnp.float32,
        )
        if d == 0:
            bret[pl.ds(pl.multiple_of(x * 192, 192), 192), :] = rows.astype(jnp.bfloat16)
        else:
            bres[quarter] = rows.astype(jnp.bfloat16)
            bret_copy(d).start()

    for d in range(1, 8):
        z_copy(d).wait_send()
    for d in range(1, 4):
        gain_copy(d).wait_send()
        btok_copy(d).wait_send()
        for k in range(2):
            x_copy(k, d).wait_send()
    for way in range(2):
        for k in range(2):
            y_copy(k, way).wait_send()
        y_forward(way).wait_send()
    for k in range(2):
        d_copy(k).wait_send()
    for k in range(3):
        w_own(k, x).wait_send()

    @pl.when(primary)
    def _():
        for k in range(3):
            w_forward(k).wait_send()
            for h in range(4):
                w_across(k, h).wait_send()

    def dispatched(q, carry):
        for j in range(4):
            if j == 0:

                @pl.when(jnp.logical_not((q == 0) & is_self))
                def _():
                    dispatch_copy(q, j).wait_send()
            else:
                dispatch_copy(q, j).wait_send()
        return carry

    lax.fori_loop(0, NQ, dispatched, 0)

    relay(0)

    place = gslot_v[...].T[:, 0:1]
    for d in range(1, 4):
        bret_copy(d).wait_recv()
    share = 1.0 / (1.0 + jnp.exp(-gate_ref[0:1, :]))
    for n, d in enumerate((0, 1, 3, 2)):
        g = (group + d) % 4
        if d > 0:
            remote(back.at[g], back.at[g], s4send.at[0], s4recv.at[g], ep, x).wait_recv()
        for h in range(3):
            sl = slice(h * 256, h * 256 + 256)
            places = (lax.broadcasted_iota(jnp.int32, (256, GT), 1) + g * GT).astype(jnp.float32)
            pick = jnp.where(places == place[sl], 1.0, 0.0).astype(jnp.bfloat16)
            total = jnp.dot(pick, back[g], preferred_element_type=jnp.float32)
            if n == 0:
                acc[sl, :] = total + share * bret[sl, :].astype(jnp.float32)
            elif n < 3:
                acc[sl, :] += total
            else:
                out_ref[sl, :] = (acc[sl, :] + total).astype(jnp.bfloat16)

    for d in range(1, 4):
        bret_copy(d).wait_send()
        m_copy(d).wait_send()
        s4_copy(d).wait_send()

    def sent(q, carry):
        for j in range(4):
            if j == 0:

                @pl.when(jnp.logical_not(stays(q)))
                def _():
                    return_copy(j, q).wait_send()
            else:
                return_copy(j, q).wait_send()
        return carry

    lax.fori_loop(0, NQ, sent, 0)


def body(
    tokens, norm_gain, routing, route_weight, w_gate, w_up, w_down, w_branch_in, w_branch_out, branch_gate
):
    bf16, f32 = jnp.bfloat16, jnp.float32
    vmem = pl.BlockSpec(memory_space=pltpu.VMEM)
    hbm = pl.BlockSpec(memory_space=pl.ANY)
    dma = pltpu.SemaphoreType.DMA
    return pl.pallas_call(
        kernel,
        out_shape=jax.ShapeDtypeStruct((T, F), bf16),
        in_specs=[hbm, hbm, vmem, vmem, hbm, hbm, hbm, hbm, hbm, vmem],
        out_specs=vmem,
        scratch_shapes=[
            pltpu.VMEM((T, F), bf16),
            pltpu.VMEM((4, 1, F), f32),
            pltpu.VMEM((NQ, BLK, F), bf16),
            pltpu.VMEM((NQ, CAP, 4 * F), bf16),
            pltpu.VMEM((3, 4, 512, 512), bf16),
            pltpu.VMEM((2, 8, 4, 2, 32, 1024), bf16),
            pltpu.VMEM((BLK, 4 * F), bf16),
            pltpu.VMEM((BLK, 512), bf16),
            pltpu.VMEM((4, NQ, CAP, F), bf16),
            pltpu.VMEM((4, MEM, CAP, F), bf16),
            pltpu.VMEM((192, 4 * F), bf16),
            pltpu.VMEM((192, 4 * F), bf16),
            pltpu.VMEM((192, 1024), bf16),
            pltpu.VMEM((4, 192, F), bf16),
            pltpu.VMEM((T, F), bf16),
            pltpu.VMEM((T, F), f32),
            pltpu.VMEM((8, T), f32),
            pltpu.VMEM((4, 8, GT), f32),
            pltpu.VMEM((4, 8, GT), f32),
            pltpu.VMEM((4, GT, T), bf16),
            pltpu.VMEM((4, GT, F), bf16),
            pltpu.VMEM((4, GT, F), bf16),
            dma((8,)),
            dma((4,)), dma((4,)),
            dma((4,)), dma((4,)),
            dma((4,)), dma((4,)),
            dma((8,)), dma((8,)),
            dma((2, 4)), dma((2, 4)),
            dma((3, 2)), dma((3, 2)),
            dma((2,)), dma((2,)),
            dma((3,)), dma((3, 4)),
            dma((3,)), dma((3, 4)),
            dma((64,)), dma((64,)),
            dma((64,)), dma((64,)),
            dma((4,)), dma((4,)),
            dma((4,)), dma((4,)),
        ],
        compiler_params=pltpu.CompilerParams(collective_id=0, has_side_effects=True, vmem_limit_bytes=60 * 1024 * 1024),
        name="layer",
    )(
        tokens,
        norm_gain.reshape(1, F),
        routing.T,
        route_weight.T,
        w_gate[0],
        w_up[0],
        w_down[0],
        w_branch_in,
        w_branch_out.T,
        branch_gate.reshape(1, F),
    )


def solution(mesh):
    return jax.shard_map(
        body,
        mesh=mesh,
        in_specs=(
            P("ep", "tp"),
            P("tp"),
            P("ep", None),
            P("ep", None),
            P("ep", "tp", None),
            P("ep", "tp", None),
            P("ep", None, "tp"),
            P("ep", "tp"),
            P("tp", "ep"),
            P("tp"),
        ),
        out_specs=P("ep", "tp"),
        check_vma=False,
    )
```

```python
import jax
import jax.numpy as jnp
from jax import lax
from jax.experimental import pallas as pl
from jax.experimental.pallas import tpu as pltpu
from jax.sharding import PartitionSpec as P

EPSILON = 1e-06
MESH = pl.DeviceIdType.MESH
CAP = 48
F = 512
T = 768
NQ = 16
BLK = 4 * CAP
GT = 384
MEM = 16
FIRST, SECOND = 6, 12


def kernel(
    tok_hbm, gain_hbm, rout_t, rw_t, wg_hbm, wu_hbm, wd_hbm, bwi_hbm, bwo_hbm, gate_ref,
    out_ref,
    tok, gains, send, land, weights, bw, normed, hidden, result, rr, btok, bnorm, bhid, bres, bret, acc, gslot_v,
    meta_out, meta, mix, rq, back,
    lsem, gsend, grecv, btsend, btrecv, brsend, brrecv, zsend, zrecv, xsend, xrecv, ysend, yrecv, dsend, drecv,
    wsend, wrecv, fsend, csend, esend, erecv, rsend, rrecv, msend, mrecv, s4send, s4recv,
):
    ep = lax.axis_index("ep")
    x = lax.axis_index("tp")
    z, y, c = ep // 8, (ep // 2) % 4, ep % 2
    m_own, s4 = ep // 4, ep % 4
    served = (ep // 2) * 2 + x // 2
    sigma = ((x % 2) * 2 + c - served % 4 + 4) % 4
    is_self = sigma == s4
    primary = x // 2 == c
    rel = (x - 2 * c + 4) % 4

    def remote(src, dst, ssem, rsem, e, xx):
        return pltpu.make_async_remote_copy(
            src_ref=src, dst_ref=dst, send_sem=ssem, recv_sem=rsem,
            device_id={"ep": e, "tp": xx}, device_id_type=MESH,
        )

    def lanes(index, width):
        return pl.ds(pl.multiple_of(index * width, width), width)

    def ep_of(zz, yy, cc):
        return (zz * 4 + yy) * 2 + cc

    def block_at(q):
        half = (q + 1) // 2
        return (m_own + 16 + half * (2 * (q % 2) - 1)) % 16

    def target_of(m, j):
        xx = (x + j) % 4
        h = 2 * (xx % 2) + (s4 + xx // 2) % 2
        r = (h - s4 + 4) % 4
        return r, m * 4 + 2 * (r // 2) + h % 2, xx

    group, mine_in = z // 2, served % MEM

    def relay_of(zz, g):
        ahead = (2 * g - zz + 16) % 8
        return jnp.where(ahead <= 3, 2 * g, 2 * g + 1), jnp.where(ahead <= 3, ahead, 7 - ahead)

    def source_z(k):
        return jnp.where(z % 2 == 0, z - k + 8, z + k) % 8

    barrier = pltpu.get_barrier_semaphore()

    def greet_one(e, xx):
        pl.semaphore_signal(barrier, inc=1, device_id={"ep": e, "tp": xx}, device_id_type=MESH)

    for d in range(1, 8):
        greet_one(ep_of((z + d) % 8, y, c), x)
    for d in range(1, 4):
        greet_one(ep, (x + d) % 4)
        greet_one(ep_of(source_z(d), y, c), x)
        greet_one(ep_of(relay_of(z, (group + d) % 4)[0], y, c), x)
    for d in (1, 3):
        greet_one(ep_of(z, (y + d) % 4, c), x)
    greet_one(ep_of(z, y, 1 - c), x)

    def greet(m, carry):
        for j in range(4):

            @pl.when(jnp.logical_not(is_self & (m == m_own) & (j == 0)))
            def _():
                greet_one(m * 4 + sigma, (x + j) % 4)

        @pl.when(jnp.logical_not(is_self & (m == mine_in)))
        def _():
            h = (s4 + m) % 4
            greet_one(group * MEM + (m // 2) * 2 + h % 2, 2 * (m % 2) + h // 2)

        return carry

    lax.fori_loop(0, NQ, greet, 0)

    loads = [
        pltpu.make_async_copy(tok_hbm, tok, lsem.at[0]),
        pltpu.make_async_copy(bwi_hbm, bw.at[0, z, y, c, :, lanes(x, 256)], lsem.at[1]),
        pltpu.make_async_copy(bwo_hbm, bw.at[1, z, y, c, :, lanes(x, 256)], lsem.at[2]),
        pltpu.make_async_copy(gain_hbm, gains.at[x], lsem.at[3]),
        pltpu.make_async_copy(tok_hbm.at[pl.ds(x * 192, 192), :], btok.at[:, lanes(x, F)], lsem.at[4]),
    ]
    for load in loads:
        load.start()
    w_hbm = (wg_hbm, wu_hbm, wd_hbm)
    w_loads = [pltpu.make_async_copy(w_hbm[k], weights.at[k, x], lsem.at[5 + k]) for k in range(3)]

    @pl.when(primary)
    def _():
        for load in w_loads:
            load.start()

    experts = lax.broadcasted_iota(jnp.int32, (64, T), 0)
    r0, r1 = rout_t[0:1, :], rout_t[1:2, :]
    named0, named1 = experts == r0, experts == r1
    gid = r0 // MEM
    in_group = lax.broadcasted_iota(jnp.int32, (16, T), 0) == gid
    one_hot = jnp.concatenate(
        [
            jnp.where(named0 | named1, 1.0, 0.0).astype(jnp.bfloat16),
            jnp.where(in_group, 1.0, 0.0).astype(jnp.bfloat16),
        ],
        axis=0,
    )
    earlier = jnp.where(
        lax.broadcasted_iota(jnp.int32, (T, T), 0) < lax.broadcasted_iota(jnp.int32, (T, T), 1), 1.0, 0.0
    ).astype(jnp.bfloat16)
    before = jnp.dot(one_hot, earlier, preferred_element_type=jnp.float32)
    pos0 = jnp.sum(jnp.where(named0, before[:64], 0.0), axis=0, keepdims=True)
    pos1 = jnp.sum(jnp.where(named1, before[:64], 0.0), axis=0, keepdims=True)
    rank = jnp.sum(jnp.where(in_group, before[64:], 0.0), axis=0, keepdims=True)
    slot0 = r0 * CAP + pos0.astype(jnp.int32)
    slot1 = r1 * CAP + pos1.astype(jnp.int32)
    gslot = (gid * GT).astype(jnp.float32) + rank
    gslot_v[...] = jnp.broadcast_to(gslot, (8, T))
    facts = jnp.concatenate(
        [
            (r0 - gid * MEM).astype(jnp.float32),
            pos0,
            (r1 - gid * MEM).astype(jnp.float32),
            pos1,
            rw_t[...],
            jnp.zeros((2, T), jnp.float32),
        ],
        axis=0,
    ).astype(jnp.bfloat16)

    for load in loads:
        load.wait()

    def dispatch_copy(q, j):
        m = block_at(q)
        r, e, xx = target_of(m, j)
        return remote(
            send.at[m, pl.ds(pl.multiple_of(r * CAP, 16), CAP), :],
            land.at[m_own, :, lanes(x, F)],
            esend.at[q * 4 + j],
            erecv.at[m_own * 4 + x],
            e,
            xx,
        )

    def pack(q, carry):
        m = block_at(q)
        slots = lax.broadcasted_iota(jnp.int32, (BLK, T), 0) + m * BLK
        pick = jnp.where((slots == slot0) | (slots == slot1), 1.0, 0.0).astype(jnp.bfloat16)
        send[m] = jnp.dot(pick, tok[...], preferred_element_type=jnp.float32).astype(jnp.bfloat16)
        return carry

    def dispatch_straight(q, carry):
        own = (q == 0) & is_self

        @pl.when(jnp.logical_not(own))
        def _():
            dispatch_copy(q, 0).start()

        @pl.when(own)
        def _():
            r, _, _ = target_of(m_own, 0)
            land[m_own, :, lanes(x, F)] = send[m_own, pl.ds(pl.multiple_of(r * CAP, 16), CAP), :]

        return carry

    def dispatch_across(q, carry):
        for j in range(1, 4):
            dispatch_copy(q, j).start()
        return carry

    pl.semaphore_wait(barrier, 13 + 6 + 64 + 16 - 2 * is_self.astype(jnp.int32))

    mate = (x + 5 - 2 * rel) % 4
    outer = (x + 3 + 2 * rel) % 4
    inner = (x + 2 * rel + 3) % 4

    def w_own(k, to):
        return remote(w_hbm[k], weights.at[k, x], wsend.at[k], wrecv.at[k, x], ep, to)

    def w_piece(k, slot, sem, e, to):
        return remote(weights.at[k, slot], weights.at[k, slot], sem, wrecv.at[k, slot], e, to)

    def w_forward(k):
        return w_piece(k, outer, fsend.at[k], ep, mate)

    def w_across(k, slot):
        return w_piece(k, slot, csend.at[k, slot], ep_of(z, y, 1 - c), x)

    def w_start(ks):
        @pl.when(primary)
        def _():
            for k in ks:
                w_own(k, mate).start()

        @pl.when(jnp.logical_not(primary))
        def _():
            for k in ks:
                w_own(k, inner).start()

    def z_copy(d):
        zz = (z + d) % 8
        mine = bw.at[:, z, y, c, :, lanes(x, 256)]
        return remote(mine, mine, zsend.at[d], zrecv.at[d], ep_of(zz, y, c), x)

    def x_copy(k, d):
        mine = bw.at[k, :, y, c, :, lanes(x, 256)]
        return remote(mine, mine, xsend.at[k, d], xrecv.at[k, d], ep, (x + d) % 4)

    def y_copy(k, way):
        mine = bw.at[k, :, y, c]
        return remote(mine, mine, ysend.at[k, way], yrecv.at[k, way], ep_of(z, (y + (1, 3)[way]) % 4, c), x)

    def y_forward(way):
        slot = (y + (3, 1)[way]) % 4
        piece = bw.at[way, :, slot, c]
        return remote(piece, piece, ysend.at[2, way], yrecv.at[2, way], ep_of(z, (y + (1, 3)[way]) % 4, c), x)

    def d_copy(k):
        mine = bw.at[k, :, :, c]
        return remote(mine, mine, dsend.at[k], drecv.at[k], ep_of(z, y, 1 - c), x)

    def gain_copy(d):
        return remote(gains.at[x], gains.at[x], gsend.at[d], grecv.at[d], ep, (x + d) % 4)

    def btok_copy(d):
        xx = (x + d) % 4
        return remote(
            tok.at[pl.ds(xx * 192, 192), :], btok.at[:, lanes(x, F)], btsend.at[d], btrecv.at[d], ep, xx
        )

    for d in range(1, 8):
        z_copy(d).start()
    for d in range(1, 4):
        gain_copy(d).start()
    w_start((0, 1))

    @pl.when(primary)
    def _():
        for k in range(3):
            w_loads[k].wait()
            w_across(k, x).start()

    def pack_and_send(q, carry):
        return dispatch_straight(q, pack(q, carry))

    lax.fori_loop(0, NQ, pack_and_send, 0)

    def w_relay(k):
        w_piece(k, outer, fsend.at[k], ep, x).wait_recv()
        w_forward(k).start()
        w_across(k, outer).start()
        w_piece(k, mate, fsend.at[k], ep, x).wait_recv()
        w_across(k, mate).start()

    def w_last(k):
        w_piece(k, (x + 2) % 4, fsend.at[k], ep, x).wait_recv()
        w_across(k, (x + 2) % 4).start()

    def w_served(k):
        for h in range(4):
            w_piece(k, h, fsend.at[k], ep, x).wait_recv()

    for d in range(1, 8):
        z_copy(d).wait_recv()
    for d in range(1, 4):
        for k in range(2):
            x_copy(k, d).start()

    lax.fori_loop(0, FIRST, dispatch_across, 0)

    def m_copy(d):
        g = (group + d) % 4
        plane, k = relay_of(z, g)
        return remote(meta_out.at[g], meta.at[k], msend.at[d], mrecv.at[k], ep_of(plane, y, c), x)

    for d in range(4):
        g = (group + d) % 4
        places = (lax.broadcasted_iota(jnp.int32, (GT, T), 0) + g * GT).astype(jnp.float32)
        pick = jnp.where(places == gslot, 1.0, 0.0).astype(jnp.bfloat16)
        told = lax.dot_general(facts, pick, (((1,), (1,)), ((), ())), preferred_element_type=jnp.float32)
        if d == 0:
            meta[0] = told
        else:
            meta_out[g] = told
            m_copy(d).start()


    @pl.when(primary)
    def _():
        for k in range(2):
            w_relay(k)

    lax.fori_loop(FIRST, SECOND, dispatch_across, 0)
    for d in range(1, 4):
        for k in range(2):
            x_copy(k, d).wait_recv()
    for way in range(2):
        for k in range(2):
            y_copy(k, way).start()
    lax.fori_loop(SECOND, NQ, dispatch_across, 0)
    w_start((2,))

    for k in range(1, 4):
        remote(meta.at[k], meta.at[k], msend.at[0], mrecv.at[k], ep, x).wait_recv()
    for k in range(4):
        columns = meta[k].T
        at0 = columns[:, 0:1] * CAP + columns[:, 1:2]
        at1 = columns[:, 2:3] * CAP + columns[:, 3:4]
        for h in range(2):
            sl = slice(h * 192, h * 192 + 192)
            slots = lax.broadcasted_iota(jnp.int32, (192, T), 1).astype(jnp.float32)
            mix[k, sl, :] = (
                jnp.where(slots == at0[sl], columns[sl, 4:5], 0.0)
                + jnp.where(slots == at1[sl], columns[sl, 5:6], 0.0)
            ).astype(jnp.bfloat16)

    @pl.when(primary)
    def _():
        w_relay(2)

    for way in range(2):
        for k in range(2):
            y_copy(k, way).wait_recv()
    for way in range(2):
        y_forward(way).start()

    @pl.when(primary)
    def _():
        for k in range(2):
            w_last(k)

    for d in range(1, 4):
        gain_copy(d).wait_recv()

    @pl.when(jnp.logical_not(primary))
    def _():
        for k in range(2):
            w_served(k)

    def norm_rows(source, target):
        floats = source.astype(jnp.float32)
        squares = jnp.sum(floats * floats, axis=1, keepdims=True)
        scaled = floats * lax.rsqrt(squares * (1.0 / (4 * F)) + EPSILON)
        for k in range(4):
            target[:, k * F : (k + 1) * F] = (scaled[:, k * F : (k + 1) * F] * gains[k]).astype(jnp.bfloat16)

    def arrival(m, xx):
        there = land.at[m, :, lanes(xx, F)]
        return remote(there, there, esend.at[0], erecv.at[m * 4 + xx], ep, xx)

    def return_copy(jj, m):
        quarter = (x + (0, 1, 3, 2)[jj]) % 4
        plane, k = relay_of(m // 2, group)
        return remote(
            result.at[quarter, m], rr.at[k, mine_in], rsend.at[jj * 16 + m], rrecv.at[k * MEM + mine_in],
            ep_of(plane, (m % 2) * 2 + sigma // 2, sigma % 2), quarter,
        )

    def stays(m):
        return is_self & (m % 2 == y // 2) & (relay_of(m // 2, group)[0] == z)

    def pair_at(i):
        return jnp.where(i == 0, 2, jnp.where(i == 1, 1, jnp.where(i == 2, 3, 0)))

    def give_back(part, jj):
        for mm in range(4):
            m = part * 4 + mm
            if jj == 0:
                own = stays(m)

                @pl.when(jnp.logical_not(own))
                def _():
                    return_copy(jj, m).start()

                @pl.when(own)
                def _():
                    rr[relay_of(m // 2, group)[1], mine_in] = result[x, m]
            else:
                return_copy(jj, m).start()

    def hide(i, carry):
        part = (z // 2 + jnp.where(i == 2, 3, jnp.where(i == 3, 2, i))) % 4
        for mm in range(4):
            m = part * 4 + mm
            for xx in range(4):

                @pl.when(jnp.logical_not(is_self & (m == m_own) & (x == xx)))
                def _():
                    arrival(m, xx).wait_recv()

        def one(r, inner):
            m, row = part * 4 + r // 3, pl.multiple_of((r % 3) * 16, 16)
            norm_rows(land[m, pl.ds(row, 16), :], normed.at[pl.ds(pl.multiple_of(r * 16, 16), 16), :])
            return inner

        lax.fori_loop(0, 12, one, 0)
        for n in range(2):
            cols = slice(n * 256, n * 256 + 256)
            sums = []
            for k in range(2):
                total = jnp.dot(normed[:, 0:F], weights[k, 0, :, cols], preferred_element_type=jnp.float32)
                for h in range(1, 4):
                    total += jnp.dot(
                        normed[:, h * F : (h + 1) * F], weights[k, h, :, cols], preferred_element_type=jnp.float32
                    )
                sums.append(total)
            gate_sum, up_sum = sums
            hidden[pl.ds(pl.multiple_of(part * BLK, BLK), BLK), cols] = (gate_sum / (1.0 + jnp.exp(-gate_sum)) * up_sum).astype(jnp.bfloat16)

        return carry

    def down(i, carry):
        part = (z // 2 + pair_at(i)) % 4
        for jj in range(4):
            quarter = (x + (0, 1, 3, 2)[jj]) % 4
            rows = jnp.dot(hidden[pl.ds(pl.multiple_of(part * BLK, BLK), BLK), :], weights[2, quarter], preferred_element_type=jnp.float32)
            result[quarter, pl.ds(part * 4, 4)] = rows.astype(jnp.bfloat16).reshape(4, CAP, F)

            @pl.when(i < 3)
            def _():
                give_back(part, jj)

        return carry

    for d in range(1, 4):
        btok_copy(d).start()
    lax.fori_loop(0, 4, hide, 0)

    @pl.when(primary)
    def _():
        w_last(2)

    @pl.when(jnp.logical_not(primary))
    def _():
        w_served(2)

    lax.fori_loop(0, 4, down, 0)

    def s4_copy(k):
        return remote(rq.at[k], back.at[group], s4send.at[k], s4recv.at[group], ep_of(source_z(k), y, c), x)

    def relay(k):
        def wait(n, inner):
            @pl.when(jnp.logical_not(is_self & (n == mine_in)))
            def _():
                remote(rr.at[k, n], rr.at[k, n], rsend.at[0], rrecv.at[k * MEM + n], ep, x).wait_recv()

            return inner

        lax.fori_loop(0, MEM, wait, 0)
        total = jnp.dot(mix[k], rr[k].reshape(T, F), preferred_element_type=jnp.float32).astype(jnp.bfloat16)
        if k == 0:
            back[group] = total
        else:
            rq[k] = total
            s4_copy(k).start()

    for d in range(1, 4):
        btok_copy(d).wait_recv()

    def branch_norm(r, carry):
        rows = pl.ds(pl.multiple_of(r * 16, 16), 16)
        norm_rows(btok[rows, :], bnorm.at[rows, :])
        return carry

    lax.fori_loop(0, 12, branch_norm, 0)

    relay(3)
    for jj in range(4):
        give_back(group, jj)
    for way in range(2):
        y_forward(way).wait_recv()
    for k in range(2):
        d_copy(k).start()
    relay(2)
    for k in range(2):
        d_copy(k).wait_recv()

    w_in = bw.at[0].reshape(2048, 1024)
    w_out = bw.at[1].reshape(2048, 1024)
    for n in range(4):
        cols = slice(n * 256, n * 256 + 256)
        total = jnp.dot(bnorm[...], w_in[:, cols], preferred_element_type=jnp.float32)
        bhid[:, cols] = (total / (1.0 + jnp.exp(-total))).astype(jnp.bfloat16)

    def bret_copy(d):
        xx = (x + d) % 4
        return remote(
            bres.at[xx], bret.at[pl.ds(x * 192, 192), :], brsend.at[d], brrecv.at[d], ep, xx
        )

    for d in (1, 3, 2, 0):
        quarter = (x + d) % 4
        rows = lax.dot_general(
            bhid[...],
            w_out[pl.ds(pl.multiple_of(quarter * F, F), F), :],
            (((1,), (1,)), ((), ())),
            preferred_element_type=jnp.float32,
        )
        if d == 0:
            bret[pl.ds(pl.multiple_of(x * 192, 192), 192), :] = rows.astype(jnp.bfloat16)
        else:
            bres[quarter] = rows.astype(jnp.bfloat16)
            bret_copy(d).start()
    relay(1)

    for d in range(1, 8):
        z_copy(d).wait_send()
    for d in range(1, 4):
        gain_copy(d).wait_send()
        btok_copy(d).wait_send()
        for k in range(2):
            x_copy(k, d).wait_send()
    for way in range(2):
        for k in range(2):
            y_copy(k, way).wait_send()
        y_forward(way).wait_send()
    for k in range(2):
        d_copy(k).wait_send()
    for k in range(3):
        w_own(k, x).wait_send()

    @pl.when(primary)
    def _():
        for k in range(3):
            w_forward(k).wait_send()
            for h in range(4):
                w_across(k, h).wait_send()

    def dispatched(q, carry):
        for j in range(4):
            if j == 0:

                @pl.when(jnp.logical_not((q == 0) & is_self))
                def _():
                    dispatch_copy(q, j).wait_send()
            else:
                dispatch_copy(q, j).wait_send()
        return carry

    lax.fori_loop(0, NQ, dispatched, 0)

    relay(0)

    place = gslot_v[...].T[:, 0:1]
    for d in range(1, 4):
        bret_copy(d).wait_recv()
    share = 1.0 / (1.0 + jnp.exp(-gate_ref[0:1, :]))
    for n, d in enumerate((0, 1, 3, 2)):
        g = (group + d) % 4
        if d > 0:
            remote(back.at[g], back.at[g], s4send.at[0], s4recv.at[g], ep, x).wait_recv()
        for h in range(3):
            sl = slice(h * 256, h * 256 + 256)
            places = (lax.broadcasted_iota(jnp.int32, (256, GT), 1) + g * GT).astype(jnp.float32)
            pick = jnp.where(places == place[sl], 1.0, 0.0).astype(jnp.bfloat16)
            total = jnp.dot(pick, back[g], preferred_element_type=jnp.float32)
            if n == 0:
                acc[sl, :] = total + share * bret[sl, :].astype(jnp.float32)
            elif n < 3:
                acc[sl, :] += total
            else:
                out_ref[sl, :] = (acc[sl, :] + total).astype(jnp.bfloat16)

    for d in range(1, 4):
        bret_copy(d).wait_send()
        m_copy(d).wait_send()
        s4_copy(d).wait_send()

    def sent(q, carry):
        for j in range(4):
            if j == 0:

                @pl.when(jnp.logical_not(stays(q)))
                def _():
                    return_copy(j, q).wait_send()
            else:
                return_copy(j, q).wait_send()
        return carry

    lax.fori_loop(0, NQ, sent, 0)


def body(
    tokens, norm_gain, routing, route_weight, w_gate, w_up, w_down, w_branch_in, w_branch_out, branch_gate
):
    bf16, f32 = jnp.bfloat16, jnp.float32
    vmem = pl.BlockSpec(memory_space=pltpu.VMEM)
    hbm = pl.BlockSpec(memory_space=pl.ANY)
    dma = pltpu.SemaphoreType.DMA
    return pl.pallas_call(
        kernel,
        out_shape=jax.ShapeDtypeStruct((T, F), bf16),
        in_specs=[hbm, hbm, vmem, vmem, hbm, hbm, hbm, hbm, hbm, vmem],
        out_specs=vmem,
        scratch_shapes=[
            pltpu.VMEM((T, F), bf16),
            pltpu.VMEM((4, 1, F), f32),
            pltpu.VMEM((NQ, BLK, F), bf16),
            pltpu.VMEM((NQ, CAP, 4 * F), bf16),
            pltpu.VMEM((3, 4, 512, 512), bf16),
            pltpu.VMEM((2, 8, 4, 2, 32, 1024), bf16),
            pltpu.VMEM((BLK, 4 * F), bf16),
            pltpu.VMEM((T, 512), bf16),
            pltpu.VMEM((4, NQ, CAP, F), bf16),
            pltpu.VMEM((4, MEM, CAP, F), bf16),
            pltpu.VMEM((192, 4 * F), bf16),
            pltpu.VMEM((192, 4 * F), bf16),
            pltpu.VMEM((192, 1024), bf16),
            pltpu.VMEM((4, 192, F), bf16),
            pltpu.VMEM((T, F), bf16),
            pltpu.VMEM((T, F), f32),
            pltpu.VMEM((8, T), f32),
            pltpu.VMEM((4, 8, GT), f32),
            pltpu.VMEM((4, 8, GT), f32),
            pltpu.VMEM((4, GT, T), bf16),
            pltpu.VMEM((4, GT, F), bf16),
            pltpu.VMEM((4, GT, F), bf16),
            dma((8,)),
            dma((4,)), dma((4,)),
            dma((4,)), dma((4,)),
            dma((4,)), dma((4,)),
            dma((8,)), dma((8,)),
            dma((2, 4)), dma((2, 4)),
            dma((3, 2)), dma((3, 2)),
            dma((2,)), dma((2,)),
            dma((3,)), dma((3, 4)),
            dma((3,)), dma((3, 4)),
            dma((64,)), dma((64,)),
            dma((64,)), dma((64,)),
            dma((4,)), dma((4,)),
            dma((4,)), dma((4,)),
        ],
        compiler_params=pltpu.CompilerParams(collective_id=0, has_side_effects=True, vmem_limit_bytes=60 * 1024 * 1024),
        name="layer",
    )(
        tokens,
        norm_gain.reshape(1, F),
        routing.T,
        route_weight.T,
        w_gate[0],
        w_up[0],
        w_down[0],
        w_branch_in,
        w_branch_out.T,
        branch_gate.reshape(1, F),
    )


def solution(mesh):
    return jax.shard_map(
        body,
        mesh=mesh,
        in_specs=(
            P("ep", "tp"),
            P("tp"),
            P("ep", None),
            P("ep", None),
            P("ep", "tp", None),
            P("ep", "tp", None),
            P("ep", None, "tp"),
            P("ep", "tp"),
            P("tp", "ep"),
            P("tp"),
        ),
        out_specs=P("ep", "tp"),
        check_vma=False,
    )
```

```python
import jax
import jax.numpy as jnp
from jax import lax
from jax.experimental import pallas as pl
from jax.experimental.pallas import tpu as pltpu
from jax.sharding import PartitionSpec as P

EPSILON = 1e-06
MESH = pl.DeviceIdType.MESH
CAP = 48
F = 512
T = 768
NQ = 16
BLK = 4 * CAP
GT = 384
MEM = 16
FIRST, SECOND = 6, 16


def kernel(
    tok_hbm, gain_hbm, rout_t, rw_t, wg_hbm, wu_hbm, wd_hbm, bwi_hbm, bwo_hbm, gate_ref,
    out_ref,
    tok, gains, send, land, weights, bw, normed, hidden, result, rr, btok, bnorm, bhid, bres, bret, acc, gslot_v,
    meta_out, meta, mix, rq, back,
    lsem, gsend, grecv, btsend, btrecv, brsend, brrecv, zsend, zrecv, xsend, xrecv, ysend, yrecv, dsend, drecv,
    wsend, wrecv, fsend, csend, esend, erecv, rsend, rrecv, msend, mrecv, s4send, s4recv,
):
    ep = lax.axis_index("ep")
    x = lax.axis_index("tp")
    z, y, c = ep // 8, (ep // 2) % 4, ep % 2
    m_own, s4 = ep // 4, ep % 4
    served = (ep // 2) * 2 + x // 2
    sigma = ((x % 2) * 2 + c - served % 4 + 4) % 4
    is_self = sigma == s4
    primary = x // 2 == c
    rel = (x - 2 * c + 4) % 4

    def remote(src, dst, ssem, rsem, e, xx):
        return pltpu.make_async_remote_copy(
            src_ref=src, dst_ref=dst, send_sem=ssem, recv_sem=rsem,
            device_id={"ep": e, "tp": xx}, device_id_type=MESH,
        )

    def lanes(index, width):
        return pl.ds(pl.multiple_of(index * width, width), width)

    def ep_of(zz, yy, cc):
        return (zz * 4 + yy) * 2 + cc

    def block_at(q):
        half = (q + 1) // 2
        return (m_own + 16 + half * (2 * (q % 2) - 1)) % 16

    def target_of(m, j):
        xx = (x + j) % 4
        h = 2 * (xx % 2) + (s4 + xx // 2) % 2
        r = (h - s4 + 4) % 4
        return r, m * 4 + 2 * (r // 2) + h % 2, xx

    group, mine_in = z // 2, served % MEM

    def relay_of(zz, g):
        ahead = (2 * g - zz + 16) % 8
        return jnp.where(ahead <= 3, 2 * g, 2 * g + 1), jnp.where(ahead <= 3, ahead, 7 - ahead)

    def source_z(k):
        return jnp.where(z % 2 == 0, z - k + 8, z + k) % 8

    barrier = pltpu.get_barrier_semaphore()

    def greet_one(e, xx):
        pl.semaphore_signal(barrier, inc=1, device_id={"ep": e, "tp": xx}, device_id_type=MESH)

    for d in range(1, 8):
        greet_one(ep_of((z + d) % 8, y, c), x)
    for d in range(1, 4):
        greet_one(ep, (x + d) % 4)
        greet_one(ep_of(source_z(d), y, c), x)
        greet_one(ep_of(relay_of(z, (group + d) % 4)[0], y, c), x)
    for d in (1, 3):
        greet_one(ep_of(z, (y + d) % 4, c), x)
    greet_one(ep_of(z, y, 1 - c), x)

    def greet(m, carry):
        for j in range(4):

            @pl.when(jnp.logical_not(is_self & (m == m_own) & (j == 0)))
            def _():
                greet_one(m * 4 + sigma, (x + j) % 4)

        @pl.when(jnp.logical_not(is_self & (m == mine_in)))
        def _():
            h = (s4 + m) % 4
            greet_one(group * MEM + (m // 2) * 2 + h % 2, 2 * (m % 2) + h // 2)

        return carry

    lax.fori_loop(0, NQ, greet, 0)

    loads = [
        pltpu.make_async_copy(tok_hbm, tok, lsem.at[0]),
        pltpu.make_async_copy(bwi_hbm, bw.at[0, z, y, c, :, lanes(x, 256)], lsem.at[1]),
        pltpu.make_async_copy(bwo_hbm, bw.at[1, z, y, c, :, lanes(x, 256)], lsem.at[2]),
        pltpu.make_async_copy(gain_hbm, gains.at[x], lsem.at[3]),
        pltpu.make_async_copy(tok_hbm.at[pl.ds(x * 192, 192), :], btok.at[:, lanes(x, F)], lsem.at[4]),
    ]
    for load in loads:
        load.start()
    w_hbm = (wg_hbm, wu_hbm, wd_hbm)
    w_loads = [pltpu.make_async_copy(w_hbm[k], weights.at[k, x], lsem.at[5 + k]) for k in range(3)]

    @pl.when(primary)
    def _():
        for load in w_loads:
            load.start()

    experts = lax.broadcasted_iota(jnp.int32, (64, T), 0)
    r0, r1 = rout_t[0:1, :], rout_t[1:2, :]
    named0, named1 = experts == r0, experts == r1
    gid = r0 // MEM
    in_group = lax.broadcasted_iota(jnp.int32, (16, T), 0) == gid
    one_hot = jnp.concatenate(
        [
            jnp.where(named0 | named1, 1.0, 0.0).astype(jnp.bfloat16),
            jnp.where(in_group, 1.0, 0.0).astype(jnp.bfloat16),
        ],
        axis=0,
    )
    earlier = jnp.where(
        lax.broadcasted_iota(jnp.int32, (T, T), 0) < lax.broadcasted_iota(jnp.int32, (T, T), 1), 1.0, 0.0
    ).astype(jnp.bfloat16)
    before = jnp.dot(one_hot, earlier, preferred_element_type=jnp.float32)
    pos0 = jnp.sum(jnp.where(named0, before[:64], 0.0), axis=0, keepdims=True)
    pos1 = jnp.sum(jnp.where(named1, before[:64], 0.0), axis=0, keepdims=True)
    rank = jnp.sum(jnp.where(in_group, before[64:], 0.0), axis=0, keepdims=True)
    slot0 = r0 * CAP + pos0.astype(jnp.int32)
    slot1 = r1 * CAP + pos1.astype(jnp.int32)
    gslot = (gid * GT).astype(jnp.float32) + rank
    gslot_v[...] = jnp.broadcast_to(gslot, (8, T))
    facts = jnp.concatenate(
        [
            (r0 - gid * MEM).astype(jnp.float32),
            pos0,
            (r1 - gid * MEM).astype(jnp.float32),
            pos1,
            rw_t[...],
            jnp.zeros((2, T), jnp.float32),
        ],
        axis=0,
    ).astype(jnp.bfloat16)

    for load in loads:
        load.wait()

    def dispatch_copy(q, j):
        m = block_at(q)
        r, e, xx = target_of(m, j)
        return remote(
            send.at[m, pl.ds(pl.multiple_of(r * CAP, 16), CAP), :],
            land.at[m_own, :, lanes(x, F)],
            esend.at[q * 4 + j],
            erecv.at[m_own * 4 + x],
            e,
            xx,
        )

    def pack(q, carry):
        m = block_at(q)
        slots = lax.broadcasted_iota(jnp.int32, (BLK, T), 0) + m * BLK
        pick = jnp.where((slots == slot0) | (slots == slot1), 1.0, 0.0).astype(jnp.bfloat16)
        send[m] = jnp.dot(pick, tok[...], preferred_element_type=jnp.float32).astype(jnp.bfloat16)
        return carry

    def dispatch_straight(q, carry):
        own = (q == 0) & is_self

        @pl.when(jnp.logical_not(own))
        def _():
            dispatch_copy(q, 0).start()

        @pl.when(own)
        def _():
            r, _, _ = target_of(m_own, 0)
            land[m_own, :, lanes(x, F)] = send[m_own, pl.ds(pl.multiple_of(r * CAP, 16), CAP), :]

        return carry

    def dispatch_across(q, carry):
        for j in range(1, 4):
            dispatch_copy(q, j).start()
        return carry

    pl.semaphore_wait(barrier, 13 + 6 + 64 + 16 - 2 * is_self.astype(jnp.int32))

    mate = (x + 5 - 2 * rel) % 4
    outer = (x + 3 + 2 * rel) % 4
    inner = (x + 2 * rel + 3) % 4

    def w_own(k, to):
        return remote(w_hbm[k], weights.at[k, x], wsend.at[k], wrecv.at[k, x], ep, to)

    def w_piece(k, slot, sem, e, to):
        return remote(weights.at[k, slot], weights.at[k, slot], sem, wrecv.at[k, slot], e, to)

    def w_forward(k):
        return w_piece(k, outer, fsend.at[k], ep, mate)

    def w_across(k, slot):
        return w_piece(k, slot, csend.at[k, slot], ep_of(z, y, 1 - c), x)

    def w_start(ks):
        @pl.when(primary)
        def _():
            for k in ks:
                w_own(k, mate).start()

        @pl.when(jnp.logical_not(primary))
        def _():
            for k in ks:
                w_own(k, inner).start()

    def z_copy(d):
        zz = (z + d) % 8
        mine = bw.at[:, z, y, c, :, lanes(x, 256)]
        return remote(mine, mine, zsend.at[d], zrecv.at[d], ep_of(zz, y, c), x)

    def x_copy(k, d):
        mine = bw.at[k, :, y, c, :, lanes(x, 256)]
        return remote(mine, mine, xsend.at[k, d], xrecv.at[k, d], ep, (x + d) % 4)

    def y_copy(k, way):
        mine = bw.at[k, :, y, c]
        return remote(mine, mine, ysend.at[k, way], yrecv.at[k, way], ep_of(z, (y + (1, 3)[way]) % 4, c), x)

    def y_forward(way):
        slot = (y + (3, 1)[way]) % 4
        piece = bw.at[way, :, slot, c]
        return remote(piece, piece, ysend.at[2, way], yrecv.at[2, way], ep_of(z, (y + (1, 3)[way]) % 4, c), x)

    def d_copy(k):
        mine = bw.at[k, :, :, c]
        return remote(mine, mine, dsend.at[k], drecv.at[k], ep_of(z, y, 1 - c), x)

    def gain_copy(d):
        return remote(gains.at[x], gains.at[x], gsend.at[d], grecv.at[d], ep, (x + d) % 4)

    def btok_copy(d):
        xx = (x + d) % 4
        return remote(
            tok.at[pl.ds(xx * 192, 192), :], btok.at[:, lanes(x, F)], btsend.at[d], btrecv.at[d], ep, xx
        )

    for d in range(1, 8):
        z_copy(d).start()
    for d in range(1, 4):
        gain_copy(d).start()
    w_start((0, 1))

    @pl.when(primary)
    def _():
        for k in range(3):
            w_loads[k].wait()
            w_across(k, x).start()

    def pack_and_send(q, carry):
        return dispatch_straight(q, pack(q, carry))

    lax.fori_loop(0, NQ, pack_and_send, 0)

    def w_relay(k):
        w_piece(k, outer, fsend.at[k], ep, x).wait_recv()
        w_forward(k).start()
        w_across(k, outer).start()
        w_piece(k, mate, fsend.at[k], ep, x).wait_recv()
        w_across(k, mate).start()

    def w_last(k):
        w_piece(k, (x + 2) % 4, fsend.at[k], ep, x).wait_recv()
        w_across(k, (x + 2) % 4).start()

    def w_served(k):
        for h in range(4):
            w_piece(k, h, fsend.at[k], ep, x).wait_recv()

    for d in range(1, 8):
        z_copy(d).wait_recv()
    for d in range(1, 4):
        for k in range(2):
            x_copy(k, d).start()

    lax.fori_loop(0, FIRST, dispatch_across, 0)

    def m_copy(d):
        g = (group + d) % 4
        plane, k = relay_of(z, g)
        return remote(meta_out.at[g], meta.at[k], msend.at[d], mrecv.at[k], ep_of(plane, y, c), x)

    for d in range(4):
        g = (group + d) % 4
        places = (lax.broadcasted_iota(jnp.int32, (GT, T), 0) + g * GT).astype(jnp.float32)
        pick = jnp.where(places == gslot, 1.0, 0.0).astype(jnp.bfloat16)
        told = lax.dot_general(facts, pick, (((1,), (1,)), ((), ())), preferred_element_type=jnp.float32)
        if d == 0:
            meta[0] = told
        else:
            meta_out[g] = told
            m_copy(d).start()


    @pl.when(primary)
    def _():
        for k in range(2):
            w_relay(k)

    lax.fori_loop(FIRST, SECOND, dispatch_across, 0)
    for d in range(1, 4):
        for k in range(2):
            x_copy(k, d).wait_recv()
    for way in range(2):
        for k in range(2):
            y_copy(k, way).start()
    lax.fori_loop(SECOND, NQ, dispatch_across, 0)
    w_start((2,))

    for k in range(1, 4):
        remote(meta.at[k], meta.at[k], msend.at[0], mrecv.at[k], ep, x).wait_recv()
    for k in range(4):
        columns = meta[k].T
        at0 = columns[:, 0:1] * CAP + columns[:, 1:2]
        at1 = columns[:, 2:3] * CAP + columns[:, 3:4]
        for h in range(2):
            sl = slice(h * 192, h * 192 + 192)
            slots = lax.broadcasted_iota(jnp.int32, (192, T), 1).astype(jnp.float32)
            mix[k, sl, :] = (
                jnp.where(slots == at0[sl], columns[sl, 4:5], 0.0)
                + jnp.where(slots == at1[sl], columns[sl, 5:6], 0.0)
            ).astype(jnp.bfloat16)

    @pl.when(primary)
    def _():
        w_relay(2)

    for way in range(2):
        for k in range(2):
            y_copy(k, way).wait_recv()
    for way in range(2):
        y_forward(way).start()

    @pl.when(primary)
    def _():
        for k in range(2):
            w_last(k)

    for d in range(1, 4):
        gain_copy(d).wait_recv()

    @pl.when(jnp.logical_not(primary))
    def _():
        for k in range(2):
            w_served(k)

    def norm_rows(source, target):
        floats = source.astype(jnp.float32)
        squares = jnp.sum(floats * floats, axis=1, keepdims=True)
        scaled = floats * lax.rsqrt(squares * (1.0 / (4 * F)) + EPSILON)
        for k in range(4):
            target[:, k * F : (k + 1) * F] = (scaled[:, k * F : (k + 1) * F] * gains[k]).astype(jnp.bfloat16)

    def arrival(m, xx):
        there = land.at[m, :, lanes(xx, F)]
        return remote(there, there, esend.at[0], erecv.at[m * 4 + xx], ep, xx)

    def return_copy(jj, m):
        quarter = (x + (0, 1, 3, 2)[jj]) % 4
        plane, k = relay_of(m // 2, group)
        return remote(
            result.at[quarter, m], rr.at[k, mine_in], rsend.at[jj * 16 + m], rrecv.at[k * MEM + mine_in],
            ep_of(plane, (m % 2) * 2 + sigma // 2, sigma % 2), quarter,
        )

    def stays(m):
        return is_self & (m % 2 == y // 2) & (relay_of(m // 2, group)[0] == z)

    def pair_at(i):
        return jnp.where(i == 0, 2, jnp.where(i == 1, 1, jnp.where(i == 2, 3, 0)))

    def give_back(part, jj):
        for mm in range(4):
            m = part * 4 + mm
            if jj == 0:
                own = stays(m)

                @pl.when(jnp.logical_not(own))
                def _():
                    return_copy(jj, m).start()

                @pl.when(own)
                def _():
                    rr[relay_of(m // 2, group)[1], mine_in] = result[x, m]
            else:
                return_copy(jj, m).start()

    def hide(i, carry):
        part = (z // 2 + jnp.where(i == 2, 3, jnp.where(i == 3, 2, i))) % 4
        for mm in range(4):
            m = part * 4 + mm
            for xx in range(4):

                @pl.when(jnp.logical_not(is_self & (m == m_own) & (x == xx)))
                def _():
                    arrival(m, xx).wait_recv()

        def one(r, inner):
            m, row = part * 4 + r // 3, pl.multiple_of((r % 3) * 16, 16)
            norm_rows(land[m, pl.ds(row, 16), :], normed.at[pl.ds(pl.multiple_of(r * 16, 16), 16), :])
            return inner

        lax.fori_loop(0, 12, one, 0)
        for n in range(2):
            cols = slice(n * 256, n * 256 + 256)
            sums = []
            for k in range(2):
                total = jnp.dot(normed[:, 0:F], weights[k, 0, :, cols], preferred_element_type=jnp.float32)
                for h in range(1, 4):
                    total += jnp.dot(
                        normed[:, h * F : (h + 1) * F], weights[k, h, :, cols], preferred_element_type=jnp.float32
                    )
                sums.append(total)
            gate_sum, up_sum = sums
            hidden[pl.ds(pl.multiple_of(part * BLK, BLK), BLK), cols] = (gate_sum / (1.0 + jnp.exp(-gate_sum)) * up_sum).astype(jnp.bfloat16)

        return carry

    def down(i, carry):
        part = (z // 2 + pair_at(i)) % 4
        for jj in range(4):
            quarter = (x + (0, 1, 3, 2)[jj]) % 4
            rows = jnp.dot(hidden[pl.ds(pl.multiple_of(part * BLK, BLK), BLK), :], weights[2, quarter], preferred_element_type=jnp.float32)
            result[quarter, pl.ds(part * 4, 4)] = rows.astype(jnp.bfloat16).reshape(4, CAP, F)

            @pl.when(i < 3)
            def _():
                give_back(part, jj)

        return carry

    for d in range(1, 4):
        btok_copy(d).start()
    lax.fori_loop(0, 4, hide, 0)

    @pl.when(primary)
    def _():
        w_last(2)

    @pl.when(jnp.logical_not(primary))
    def _():
        w_served(2)

    lax.fori_loop(0, 4, down, 0)

    def s4_copy(k):
        return remote(rq.at[k], back.at[group], s4send.at[k], s4recv.at[group], ep_of(source_z(k), y, c), x)

    def relay(k):
        def wait(n, inner):
            @pl.when(jnp.logical_not(is_self & (n == mine_in)))
            def _():
                remote(rr.at[k, n], rr.at[k, n], rsend.at[0], rrecv.at[k * MEM + n], ep, x).wait_recv()

            return inner

        lax.fori_loop(0, MEM, wait, 0)
        total = jnp.dot(mix[k], rr[k].reshape(T, F), preferred_element_type=jnp.float32).astype(jnp.bfloat16)
        if k == 0:
            back[group] = total
        else:
            rq[k] = total
            s4_copy(k).start()

    for d in range(1, 4):
        btok_copy(d).wait_recv()

    def branch_norm(r, carry):
        rows = pl.ds(pl.multiple_of(r * 16, 16), 16)
        norm_rows(btok[rows, :], bnorm.at[rows, :])
        return carry

    lax.fori_loop(0, 12, branch_norm, 0)

    relay(3)
    for jj in range(4):
        give_back(group, jj)
    for way in range(2):
        y_forward(way).wait_recv()
    for k in range(2):
        d_copy(k).start()
    relay(2)
    for k in range(2):
        d_copy(k).wait_recv()

    w_in = bw.at[0].reshape(2048, 1024)
    w_out = bw.at[1].reshape(2048, 1024)
    for n in range(4):
        cols = slice(n * 256, n * 256 + 256)
        total = jnp.dot(bnorm[...], w_in[:, cols], preferred_element_type=jnp.float32)
        bhid[:, cols] = (total / (1.0 + jnp.exp(-total))).astype(jnp.bfloat16)

    def bret_copy(d):
        xx = (x + d) % 4
        return remote(
            bres.at[xx], bret.at[pl.ds(x * 192, 192), :], brsend.at[d], brrecv.at[d], ep, xx
        )

    for d in (1, 3, 2, 0):
        quarter = (x + d) % 4
        rows = lax.dot_general(
            bhid[...],
            w_out[pl.ds(pl.multiple_of(quarter * F, F), F), :],
            (((1,), (1,)), ((), ())),
            preferred_element_type=jnp.float32,
        )
        if d == 0:
            bret[pl.ds(pl.multiple_of(x * 192, 192), 192), :] = rows.astype(jnp.bfloat16)
        else:
            bres[quarter] = rows.astype(jnp.bfloat16)
            bret_copy(d).start()
    relay(1)

    for d in range(1, 8):
        z_copy(d).wait_send()
    for d in range(1, 4):
        gain_copy(d).wait_send()
        btok_copy(d).wait_send()
        for k in range(2):
            x_copy(k, d).wait_send()
    for way in range(2):
        for k in range(2):
            y_copy(k, way).wait_send()
        y_forward(way).wait_send()
    for k in range(2):
        d_copy(k).wait_send()
    for k in range(3):
        w_own(k, x).wait_send()

    @pl.when(primary)
    def _():
        for k in range(3):
            w_forward(k).wait_send()
            for h in range(4):
                w_across(k, h).wait_send()

    def dispatched(q, carry):
        for j in range(4):
            if j == 0:

                @pl.when(jnp.logical_not((q == 0) & is_self))
                def _():
                    dispatch_copy(q, j).wait_send()
            else:
                dispatch_copy(q, j).wait_send()
        return carry

    lax.fori_loop(0, NQ, dispatched, 0)

    relay(0)

    place = gslot_v[...].T[:, 0:1]
    for d in range(1, 4):
        bret_copy(d).wait_recv()
    share = 1.0 / (1.0 + jnp.exp(-gate_ref[0:1, :]))
    for n, d in enumerate((0, 1, 3, 2)):
        g = (group + d) % 4
        if d > 0:
            remote(back.at[g], back.at[g], s4send.at[0], s4recv.at[g], ep, x).wait_recv()
        for h in range(3):
            sl = slice(h * 256, h * 256 + 256)
            places = (lax.broadcasted_iota(jnp.int32, (256, GT), 1) + g * GT).astype(jnp.float32)
            pick = jnp.where(places == place[sl], 1.0, 0.0).astype(jnp.bfloat16)
            total = jnp.dot(pick, back[g], preferred_element_type=jnp.float32)
            if n == 0:
                acc[sl, :] = total + share * bret[sl, :].astype(jnp.float32)
            elif n < 3:
                acc[sl, :] += total
            else:
                out_ref[sl, :] = (acc[sl, :] + total).astype(jnp.bfloat16)

    for d in range(1, 4):
        bret_copy(d).wait_send()
        m_copy(d).wait_send()
        s4_copy(d).wait_send()

    def sent(q, carry):
        for j in range(4):
            if j == 0:

                @pl.when(jnp.logical_not(stays(q)))
                def _():
                    return_copy(j, q).wait_send()
            else:
                return_copy(j, q).wait_send()
        return carry

    lax.fori_loop(0, NQ, sent, 0)


def body(
    tokens, norm_gain, routing, route_weight, w_gate, w_up, w_down, w_branch_in, w_branch_out, branch_gate
):
    bf16, f32 = jnp.bfloat16, jnp.float32
    vmem = pl.BlockSpec(memory_space=pltpu.VMEM)
    hbm = pl.BlockSpec(memory_space=pl.ANY)
    dma = pltpu.SemaphoreType.DMA
    return pl.pallas_call(
        kernel,
        out_shape=jax.ShapeDtypeStruct((T, F), bf16),
        in_specs=[hbm, hbm, vmem, vmem, hbm, hbm, hbm, hbm, hbm, vmem],
        out_specs=vmem,
        scratch_shapes=[
            pltpu.VMEM((T, F), bf16),
            pltpu.VMEM((4, 1, F), f32),
            pltpu.VMEM((NQ, BLK, F), bf16),
            pltpu.VMEM((NQ, CAP, 4 * F), bf16),
            pltpu.VMEM((3, 4, 512, 512), bf16),
            pltpu.VMEM((2, 8, 4, 2, 32, 1024), bf16),
            pltpu.VMEM((BLK, 4 * F), bf16),
            pltpu.VMEM((T, 512), bf16),
            pltpu.VMEM((4, NQ, CAP, F), bf16),
            pltpu.VMEM((4, MEM, CAP, F), bf16),
            pltpu.VMEM((192, 4 * F), bf16),
            pltpu.VMEM((192, 4 * F), bf16),
            pltpu.VMEM((192, 1024), bf16),
            pltpu.VMEM((4, 192, F), bf16),
            pltpu.VMEM((T, F), bf16),
            pltpu.VMEM((T, F), f32),
            pltpu.VMEM((8, T), f32),
            pltpu.VMEM((4, 8, GT), f32),
            pltpu.VMEM((4, 8, GT), f32),
            pltpu.VMEM((4, GT, T), bf16),
            pltpu.VMEM((4, GT, F), bf16),
            pltpu.VMEM((4, GT, F), bf16),
            dma((8,)),
            dma((4,)), dma((4,)),
            dma((4,)), dma((4,)),
            dma((4,)), dma((4,)),
            dma((8,)), dma((8,)),
            dma((2, 4)), dma((2, 4)),
            dma((3, 2)), dma((3, 2)),
            dma((2,)), dma((2,)),
            dma((3,)), dma((3, 4)),
            dma((3,)), dma((3, 4)),
            dma((64,)), dma((64,)),
            dma((64,)), dma((64,)),
            dma((4,)), dma((4,)),
            dma((4,)), dma((4,)),
        ],
        compiler_params=pltpu.CompilerParams(collective_id=0, has_side_effects=True, vmem_limit_bytes=60 * 1024 * 1024),
        name="layer",
    )(
        tokens,
        norm_gain.reshape(1, F),
        routing.T,
        route_weight.T,
        w_gate[0],
        w_up[0],
        w_down[0],
        w_branch_in,
        w_branch_out.T,
        branch_gate.reshape(1, F),
    )


def solution(mesh):
    return jax.shard_map(
        body,
        mesh=mesh,
        in_specs=(
            P("ep", "tp"),
            P("tp"),
            P("ep", None),
            P("ep", None),
            P("ep", "tp", None),
            P("ep", "tp", None),
            P("ep", None, "tp"),
            P("ep", "tp"),
            P("tp", "ep"),
            P("tp"),
        ),
        out_specs=P("ep", "tp"),
        check_vma=False,
    )
```
